512 devices in a mesh: fs: 64 (over z, y), tp: 8 (over x, core).
Axes of the slice: x: 4, y: 4, z: 16, core: 2. Of those that a mesh axis runs over, the one named last changes fastest.
Arguments:
- cotangent: bfloat16 [8192, 2048], P('fs')
- values_first: bfloat16 [8192, 2048], P('fs', 'tp'), may hold values from -6 to 6
- values_second: bfloat16 [8192, 2048], P('fs', 'tp'), may hold values from -6 to 6
- head_lambda: float32 [16], P('tp'), may hold values from 0.3 to 0.8
- out_gain: float32 [128], replicated, may hold values from 0.3 to 3
- weight: float32 [2048, 2048], P('fs', 'tp'), may hold values from -0.125 to 0.125
- left_stat: float32 [2048, 2048], P('fs', 'tp'), as said below
- right_stat: float32 [16, 128, 128], P('tp')
- left_root: bfloat16 [2048, 2048], P('fs'), as said below
- right_root: bfloat16 [16, 128, 128], P('tp')
Outputs:
- update_step: float32 [2048, 2048], P('fs', 'tp')
- new_weight: float32 [2048, 2048], P('fs', 'tp')
- new_copy: bfloat16 [2048, 2048], P(None, 'tp')
- new_left_stat: float32 [2048, 2048], P('fs', 'tp')
- new_right_stat: float32 [16, 128, 128], P('tp')
The draws below stay inside these ranges and needn't reach their ends.
Inputs may be any that keep to these rules, and one draw needn't show every extreme that they name: `left_root`: each of the 2048 x 2048 matrix and the 16 matrices of size 128 equals its transpose; the same holds for right_root. `left_stat`: the matrix and each of the 16 matrices equals its transpose; the same holds for right_stat.
All inputs are finite; a program needn't handle non-finite values.
Results may differ from the reference program's by a relative error of at most 0.007.
Values may be sent and summed in bfloat16 or wider, within the bound.
A program may use at most 64 MiB of HBM per device.

```python
import math
import jax
import jax.numpy as jnp
from jax import lax

D = 2048
HEADS = 16
VH = 128
V = 2048
TOKENS = 8192


def symmetric_blocks(key, order, spread, count):
    first_key, second_key = jax.random.split(key)
    random_part = jax.random.normal(first_key, (count, order, order), jnp.float32)
    mirrored = (random_part + jnp.swapaxes(random_part, 1, 2)) * (spread / math.sqrt(2.0 * order))
    diagonal = jnp.exp(jax.random.uniform(second_key, (count, order), jnp.float32, math.log(0.5), math.log(2.0)))
    return mirrored + diagonal[:, :, None] * jnp.eye(order, dtype=jnp.float32)[None]


def draw_left_root(key, part):
    return symmetric_blocks(jax.random.fold_in(key, 11), D, 0.5, 1)[0].astype(jnp.bfloat16)


def draw_right_root(key, part):
    return symmetric_blocks(jax.random.fold_in(key, 12), VH, 0.5, HEADS).astype(jnp.bfloat16)


def draw_left_stat(key, part):
    return symmetric_blocks(jax.random.fold_in(key, 13), D, 0.4, 1)[0]


def draw_right_stat(key, part):
    return symmetric_blocks(jax.random.fold_in(key, 14), VH, 0.4, HEADS)


def draw_cotangent(key, part):
    first_key, second_key = jax.random.split(jax.random.fold_in(key, 15), 2)
    position = jnp.arange(D, dtype=jnp.float32) / D
    rough = jnp.exp(jax.random.uniform(second_key, (D,), jnp.float32, -0.4, 0.4))
    columns = 3.0 ** position * rough
    entries = jax.random.normal(first_key, (TOKENS, D), jnp.float32)
    return (entries * columns[None, :] * (3.2 / math.sqrt(TOKENS))).astype(jnp.bfloat16)


def level_of(rng, dims, pieces, smallest, high):
    level, own = 1.0, jax.random.fold_in(rng, 6)
    for dim, parts in pieces:
        draws = jnp.exp(jax.random.uniform(jax.random.fold_in(own, dim), (parts,), jnp.float32, smallest / len(pieces), high / len(pieces)))
        level = level * jnp.repeat(draws, dims[dim] // parts).reshape([-1 if axis == dim else 1 for axis in range(len(dims))])
    return level


def gaussian(stream_key, extent, width, reach, cuts=(), kind=jnp.bfloat16):
    result = width * jax.random.normal(stream_key, extent, jnp.float32)
    if cuts:
        result = result * level_of(stream_key, extent, cuts, -0.22, 0.18)
    return jnp.clip(result, -reach, reach).astype(kind)


def setup_inputs(seed: int = 0) -> dict:
    arg_keys = jax.random.split(jax.random.key(seed), 11)
    return {
        "cotangent": draw_cotangent(jax.random.fold_in(arg_keys[10], 71), 0),
        "values_first": gaussian(arg_keys[1], (TOKENS, V), 1.0, 6.0, ((0, 64), (1, 8))),
        "values_second": gaussian(arg_keys[2], (TOKENS, V), 1.0, 6.0, ((0, 64), (1, 8))),
        "head_lambda": jnp.clip(0.3 + 0.5 * jax.random.uniform(arg_keys[3], (HEADS,), jnp.float32) ** level_of(arg_keys[3], (HEADS,), ((0, 8),), -0.2, 0.2), 0.3, 0.8),
        "out_gain": jnp.clip(jnp.exp(jax.random.uniform(arg_keys[4], (VH,), jnp.float32, math.log(0.3), math.log(3.0))), 0.3, 3.0),
        "weight": gaussian(arg_keys[5], (D, V), V ** -0.5, 0.125, ((0, 64), (1, 8)), jnp.float32),
        "left_stat": draw_left_stat(jax.random.fold_in(arg_keys[10], 71), 0),
        "right_stat": draw_right_stat(jax.random.fold_in(arg_keys[10], 71), 0),
        "left_root": draw_left_root(jax.random.fold_in(arg_keys[10], 71), 0),
        "right_root": draw_right_root(jax.random.fold_in(arg_keys[10], 71), 0),
    }


epsilon = 1e-06
decay_rate = 0.9
learn_rate = 0.01
output_scale = 0.2

def reference(cotangent, values_first, values_second, head_lambda, out_gain, weight, left_stat, right_stat, left_root, right_root):
    first = values_first.astype(jnp.float32).reshape(-1, HEADS, VH)
    second = values_second.astype(jnp.float32).reshape(-1, HEADS, VH)
    difference = first - head_lambda[None, :, None] * second
    inverse = lax.rsqrt(lax.optimization_barrier(jnp.mean(difference * difference, axis=-1, keepdims=True)) + epsilon)
    head_out = (difference * inverse * out_gain * output_scale).reshape(-1, HEADS * VH).astype(jnp.bfloat16)
    gradient = lax.dot_general(cotangent, head_out, (((0,), (0,)), ((), ())), preferred_element_type=jnp.float32)
    grad_half = gradient.astype(jnp.bfloat16)
    left_product = lax.dot_general(grad_half, grad_half, (((1,), (1,)), ((), ())), preferred_element_type=jnp.float32)
    new_left_stat = decay_rate * left_stat + (1.0 - decay_rate) / (HEADS * VH) * left_product
    heads = grad_half.astype(jnp.float32).reshape(D, HEADS, VH)
    right_product = jnp.einsum('dhi,dhj->hij', heads, heads)
    new_right_stat = decay_rate * right_stat + (1.0 - decay_rate) / D * right_product
    left_part = jnp.dot(left_root, grad_half, preferred_element_type=jnp.float32).astype(jnp.bfloat16)
    precond = jnp.einsum('dhi,hij->dhj', left_part.astype(jnp.float32).reshape(D, HEADS, VH), right_root.astype(jnp.float32)).reshape(D, HEADS * VH)
    grad_square = jnp.sum(gradient * gradient)
    update_square = jnp.sum(precond * precond)
    factor = jnp.sqrt((grad_square + epsilon) / (update_square + epsilon))
    update_step = factor * precond
    new_weight = weight - learn_rate * update_step
    return (update_step, new_weight, new_weight.astype(jnp.bfloat16), new_left_stat, new_right_stat)
```

```python
import jax
import jax.numpy as jnp
from jax import lax
from jax.experimental import pallas as pl
from jax.experimental.pallas import tpu as pltpu
from jax.sharding import Mesh
from jax.sharding import PartitionSpec as P

TP = ("tp_0", "tp_1")
FS = ("fs_0", "fs_1")
NZ, NY, NX, NC = 16, 4, 4, 2
NTP = NX * NC
ROWS = 32
COLS = 256
HEAD = 128
WIDTH = 2048
REACH = 4
FAR = (8, 7, 9, 6, 10, 5, 11)
NEAR = (3, 13, 2, 14, 1, 15)
ORDER = FAR + (4, 12) + NEAR + (0,)

epsilon = 1e-06
decay_rate = 0.9
learn_rate = 0.01
output_scale = 0.2

BF = jnp.bfloat16
F32 = jnp.float32


def rows_of(z, y):
    return pl.ds(pl.multiple_of(z * (NY * ROWS) + y * ROWS, ROWS), ROWS)


def around(position, step, size):
    return lax.rem(position + (step % size), size)


def send(src, dst, send_sem, recv_sem, device):
    return pltpu.make_async_remote_copy(
        src_ref=src,
        dst_ref=dst,
        send_sem=send_sem,
        recv_sem=recv_sem,
        device_id=device,
        device_id_type=pl.DeviceIdType.MESH,
    )


class Spread:
    def __init__(self, buf, place, sems, at):
        self.buf, self.place = buf, place
        self.zs, self.zr, self.ys, self.yr = sems
        self.at = at
        self.open = []

    def block(self, step):
        z, y, x, c = self.at
        return self.buf.at[self.place(around(z, -step, NZ), y)]

    def hop(self, step, reach, down):
        z, y, x, c = self.at
        there = around(z, -reach if down else reach, NZ)
        arrives = (step - reach if down else step + reach) % NZ
        block = self.block(step)
        return send(block, block, self.zs.at[arrives], self.zr.at[arrives], (there, y, x, c))

    def launch(self, step, reaches, down):
        for reach in reaches:
            copy = self.hop(step, reach, down)
            copy.start()
            self.open.append(copy)

    def begin(self):
        for reach in (4, 3, 2, 1):
            self.launch(0, (reach,), False)
            self.launch(0, (reach,), True)

    def wait(self, step):
        block = self.block(step)
        z, y, x, c = self.at
        send(block, block, self.zs.at[step], self.zr.at[step], (around(z, 1, NZ), y, x, c)).wait_recv()

    def relay(self):
        self.launch(4, (4, 3, 2, 1), False)
        self.launch(12, (3, 2, 1), True)

    def across(self, step):
        z, y, x, c = self.at
        block = self.block(step)
        for far in (2, 1, 3):
            copy = send(block, block, self.ys.at[far, step], self.yr.at[far, step], (z, around(y, far, NY), x, c))
            copy.start()
            self.open.append(copy)

    def wait_across(self):
        z, y, x, c = self.at
        for step in range(NZ):
            for far in (1, 2, 3):
                block = self.buf.at[self.place(around(z, -step, NZ), around(y, -far, NY))]
                send(
                    block, block, self.ys.at[far, step], self.yr.at[far, step], (z, around(y, far, NY), x, c)
                ).wait_recv()

    def drain(self):
        for copy in self.open:
            copy.wait_send()


def kernel(
    cot,
    first,
    second,
    lam,
    gain,
    weight,
    left_stat,
    right_stat,
    left_root,
    right_root,
    update_step,
    new_weight,
    new_copy,
    new_left_stat,
    new_right_stat,
    head_out,
    partial,
    partial_half,
    from_y,
    to_z,
    from_z1,
    from_z2,
    held_weight,
    portion,
    held_step,
    stat_out,
    stat_in,
    scal_z,
    scal_y,
    scal_t,
    rys,
    ryr,
    rzs,
    rzr,
    r2s,
    r2r,
    wzs,
    wzr,
    wys,
    wyr,
    gzs,
    gzr,
    gys,
    gyr,
    pzs,
    pzr,
    pys,
    pyr,
    szs,
    szr,
    sys_,
    syr,
    sts,
    str_,
    lts,
    ltr,
):
    z, y, x, c = (lax.axis_index(a) for a in ("fs_0", "fs_1", "tp_0", "tp_1"))
    at = (z, y, x, c)
    me = x * NC + c

    def z_device(step):
        return (around(z, step, NZ), y, x, c)

    def y_device(step):
        return (z, around(y, step, NY), x, c)

    def t_index(step):
        return around(me, step, NTP)

    def t_device(step):
        other = t_index(step)
        return (z, y, other // NC, lax.rem(other, NC))

    barrier = pltpu.get_barrier_semaphore()
    peers = [z_device(s) for s in (1, 2, 3, 4, 12, 13, 14, 15)]
    peers += [y_device(s) for s in (1, 2, 3)]
    peers += [t_device(s) for s in range(1, NTP)]
    for peer in peers:
        pl.semaphore_signal(barrier, inc=1, device_id=peer, device_id_type=pl.DeviceIdType.MESH)

    held_weight[rows_of(z, y)] = weight[...].astype(BF)
    for h in range(COLS // HEAD):
        lanes = slice(h * HEAD, (h + 1) * HEAD)
        difference = first[:, lanes].astype(F32) - lam[h] * second[:, lanes].astype(F32)
        mean = jnp.mean(difference * difference, axis=-1, keepdims=True)
        scaled = difference * lax.rsqrt(mean + epsilon) * gain[...] * output_scale
        head_out[:, lanes] = scaled.astype(BF)

    pl.semaphore_wait(barrier, len(peers))

    def by_rows(zz, yy):
        return rows_of(zz, yy)

    weights = Spread(held_weight, by_rows, (wzs, wzr, wys, wyr), at)
    weights.begin()

    drain = []
    for step in ORDER:
        zz = around(z, step, NZ)
        tokens = cot[:, pl.ds(pl.multiple_of(zz * HEAD, HEAD), HEAD)]
        block = lax.dot_general(
            tokens, head_out[...], (((0,), (0,)), ((), ())), preferred_element_type=F32
        )
        rows = pl.ds(pl.multiple_of(zz * HEAD, HEAD), HEAD)
        partial[rows] = block
        partial_half[rows] = block.astype(BF)
        for far in (2, 1, 3):
            copy = send(
                partial_half.at[rows_of(zz, around(y, far, NY))],
                from_y.at[far, step],
                rys.at[far, step],
                ryr.at[far, step],
                y_device(far),
            )
            copy.start()
            drain.append(copy)

    def summed(step):
        zz = around(z, step, NZ)
        total = partial[rows_of(zz, y)]
        for far in (1, 3, 2):
            send(
                from_y.at[far, step], from_y.at[far, step], rys.at[far, step], ryr.at[far, step], y_device(far)
            ).wait_recv()
            total = total + from_y[far, step].astype(F32)
        return total

    for step in FAR:
        to_z[step] = summed(step).astype(BF)
        via = step - REACH if step <= NZ // 2 else step + REACH
        copy = send(to_z.at[step], from_z1.at[via], rzs.at[step], rzr.at[via], z_device(via))
        copy.start()
        drain.append(copy)
    for step in NEAR:
        to_z[step] = summed(step).astype(BF)
        copy = send(to_z.at[step], from_z2.at[step], r2s.at[step], r2r.at[step], z_device(step))
        copy.start()
        drain.append(copy)
    for step in (0, 1, 15, 2, 14, 3, 13):
        if step:
            weights.wait(step)
        weights.across(step)
    weights.wait(4)
    weights.wait(12)
    weights.relay()
    for step, vias in ((4, (4, 3, 2, 1)), (12, (13, 14, 15))):
        total = summed(step)
        for via in sorted(vias, key=lambda v: min(v, NZ - v)):
            send(to_z.at[via], from_z1.at[via], rzs.at[via], rzr.at[via], z_device(via)).wait_recv()
            total = total + from_z1[via].astype(F32)
        to_z[step] = total.astype(BF)
        copy = send(to_z.at[step], from_z2.at[step], r2s.at[step], r2r.at[step], z_device(step))
        copy.start()
        drain.append(copy)
    own = summed(0)
    weights.across(4)
    weights.across(12)
    for step in (5, 11, 6, 10, 7, 9, 8):
        weights.wait(step)
        weights.across(step)
    for step in (1, 15, 2, 14, 3, 13, 4, 12):
        send(to_z.at[step], from_z2.at[step], r2s.at[step], r2r.at[step], z_device(step)).wait_recv()
        own = own + from_z2[step].astype(F32)

    own_half = own.astype(BF)
    portion[rows_of(z, y)] = own_half
    grads = Spread(portion, by_rows, (gzs, gzr, gys, gyr), at)
    grads.begin()
    grads.across(0)
    grad_square = jnp.sum(own * own, axis=(0, 1), keepdims=True)
    for step in (1, 15, 2, 14, 3, 13):
        grads.wait(step)
        grads.across(step)
    grads.wait(4)
    grads.wait(12)
    grads.relay()
    grads.across(4)
    grads.across(12)
    for step in (5, 11, 6, 10, 7, 9, 8):
        grads.wait(step)
        grads.across(step)
    grads.wait_across()

    left_half = jnp.dot(left_root[...], portion[...], preferred_element_type=F32).astype(BF)
    steps = [
        jnp.dot(left_half[:, h * HEAD : (h + 1) * HEAD], right_root[h], preferred_element_type=F32)
        for h in range(COLS // HEAD)
    ]
    precond = jnp.concatenate(steps, axis=1)
    held_step[rows_of(z, y)] = precond.astype(BF)
    places = Spread(held_step, by_rows, (pzs, pzr, pys, pyr), at)
    places.begin()
    places.across(0)
    step_square = jnp.sum(precond * precond, axis=(0, 1), keepdims=True)
    top = lax.broadcasted_iota(jnp.int32, (8, HEAD), 0) < 4
    scal_z[z] = jnp.where(top, jnp.broadcast_to(step_square, (8, HEAD)), jnp.broadcast_to(grad_square, (8, HEAD)))
    scalars = Spread(scal_z, lambda zz, yy: zz, (szs, szr, None, None), at)
    scalars.begin()

    for j in range(NTP):
        stat_out[j] = lax.dot_general(
            own_half,
            portion[j * COLS : (j + 1) * COLS],
            (((1,), (1,)), ((), ())),
            preferred_element_type=F32,
        )
    for far in range(1, NTP):
        copy = send(
            stat_out.at[t_index(far)], stat_in.at[far], lts.at[far], ltr.at[far], t_device(far)
        )
        copy.start()
        drain.append(copy)
    for h in range(COLS // HEAD):
        lanes = slice(h * HEAD, (h + 1) * HEAD)
        product = lax.dot_general(
            portion[:, lanes], portion[:, lanes], (((0,), (0,)), ((), ())), preferred_element_type=F32
        )
        new_right_stat[h] = decay_rate * right_stat[h] + (1.0 - decay_rate) / WIDTH * product

    for step in (1, 15, 2, 14, 3, 13):
        places.wait(step)
        places.across(step)
    places.wait(4)
    places.wait(12)
    places.relay()
    scalars.wait(4)
    scalars.wait(12)
    scalars.relay()
    places.across(4)
    places.across(12)
    stat = stat_out[me]
    for far in range(1, NTP):
        send(
            stat_out.at[t_index(far)], stat_in.at[far], lts.at[far], ltr.at[far], t_device(far)
        ).wait_recv()
        stat = stat + stat_in[far]
    new_left_stat[...] = decay_rate * left_stat[...] + (1.0 - decay_rate) / WIDTH * stat
    for step in (5, 11, 6, 10, 7, 9, 8):
        places.wait(step)
        places.across(step)
    for step in (1, 15, 2, 14, 3, 13, 5, 11, 6, 10, 7, 9, 8):
        scalars.wait(step)
    total = scal_z[0]
    for k in range(1, NZ):
        total = total + scal_z[k]
    scal_y[y] = total
    for far in (2, 1, 3):
        copy = send(scal_y.at[y], scal_y.at[y], sys_.at[far], syr.at[far], y_device(far))
        copy.start()
        drain.append(copy)
    for far in (1, 3, 2):
        block = scal_y.at[around(y, -far, NY)]
        send(block, block, sys_.at[far], syr.at[far], y_device(far)).wait_recv()
    total = scal_y[0]
    for k in range(1, NY):
        total = total + scal_y[k]
    scal_t[me] = total
    for far in range(1, NTP):
        copy = send(scal_t.at[me], scal_t.at[me], sts.at[far], str_.at[far], t_device(far))
        copy.start()
        drain.append(copy)
    for far in range(1, NTP):
        block = scal_t.at[t_index(-far)]
        send(block, block, sts.at[far], str_.at[far], t_device(far)).wait_recv()
    total = scal_t[0]
    for k in range(1, NTP):
        total = total + scal_t[k]
    factor = jnp.sqrt((total[4:5, 0:1] + epsilon) / (total[0:1, 0:1] + epsilon))

    step_own = factor * precond
    update_step[...] = step_own
    new_weight[...] = weight[...] - learn_rate * step_own
    weights.wait_across()
    places.wait_across()
    scale = learn_rate * factor
    for k in range(NZ):
        rows = pl.ds(k * HEAD, HEAD)
        new_copy[rows] = (held_weight[rows].astype(F32) - scale * held_step[rows].astype(F32)).astype(BF)

    for copy in drain:
        copy.wait_send()
    for spread in (weights, grads, places, scalars):
        spread.drain()


def shards(
    cotangent,
    values_first,
    values_second,
    head_lambda,
    out_gain,
    weight,
    left_stat,
    right_stat,
    left_root,
    right_root,
):
    vmem = pl.BlockSpec(memory_space=pltpu.VMEM)
    smem = pl.BlockSpec(memory_space=pltpu.SMEM)
    dma = pltpu.SemaphoreType.DMA
    spread = [dma((NZ,)), dma((NZ,)), dma((NY, NZ)), dma((NY, NZ))]
    return pl.pallas_call(
        kernel,
        out_shape=(
            jax.ShapeDtypeStruct((ROWS, COLS), F32),
            jax.ShapeDtypeStruct((ROWS, COLS), F32),
            jax.ShapeDtypeStruct((WIDTH, COLS), BF),
            jax.ShapeDtypeStruct((ROWS, COLS), F32),
            jax.ShapeDtypeStruct((COLS // HEAD, HEAD, HEAD), F32),
        ),
        in_specs=[vmem, vmem, vmem, smem] + [vmem] * 6,
        out_specs=[vmem] * 5,
        scratch_shapes=[
            pltpu.VMEM((128, COLS), BF),
            pltpu.VMEM((WIDTH, COLS), F32),
            pltpu.VMEM((WIDTH, COLS), BF),
            pltpu.VMEM((NY, NZ, ROWS, COLS), BF),
            pltpu.VMEM((NZ, ROWS, COLS), BF),
            pltpu.VMEM((NZ, ROWS, COLS), BF),
            pltpu.VMEM((NZ, ROWS, COLS), BF),
            pltpu.VMEM((WIDTH, COLS), BF),
            pltpu.VMEM((WIDTH, COLS), BF),
            pltpu.VMEM((WIDTH, COLS), BF),
            pltpu.VMEM((NTP, ROWS, COLS), F32),
            pltpu.VMEM((NTP, ROWS, COLS), F32),
            pltpu.VMEM((NZ, 8, HEAD), F32),
            pltpu.VMEM((NY, 8, HEAD), F32),
            pltpu.VMEM((NTP, 8, HEAD), F32),
            dma((NY, NZ)),
            dma((NY, NZ)),
            dma((NZ,)),
            dma((NZ,)),
            dma((NZ,)),
            dma((NZ,)),
            *spread,
            *spread,
            *spread,
            dma((NZ,)),
            dma((NZ,)),
            dma((NY,)),
            dma((NY,)),
            dma((NTP,)),
            dma((NTP,)),
            dma((NTP,)),
            dma((NTP,)),
        ],
        compiler_params=pltpu.CompilerParams(collective_id=0, has_side_effects=True),
        name="fused",
    )(
        cotangent,
        values_first,
        values_second,
        head_lambda,
        out_gain.reshape(1, HEAD),
        weight,
        left_stat,
        right_stat,
        left_root,
        right_root,
    )


def solution(mesh):
    finer = Mesh(mesh.devices.reshape(NZ, NY, NX, NC), ("fs_0", "fs_1", "tp_0", "tp_1"))
    in_specs = (
        P(FS, None),
        P(FS, TP),
        P(FS, TP),
        P(TP),
        P(),
        P(FS, TP),
        P(FS, TP),
        P(TP, None, None),
        P(FS, None),
        P(TP, None, None),
    )
    out_specs = (P(FS, TP), P(FS, TP), P(None, TP), P(FS, TP), P(TP, None, None))
    return jax.shard_map(
        shards, mesh=finer, in_specs=in_specs, out_specs=out_specs, check_vma=False
    )
```

```python
import jax
import jax.numpy as jnp
from jax import lax
from jax.experimental import pallas as pl
from jax.experimental.pallas import tpu as pltpu
from jax.sharding import Mesh
from jax.sharding import PartitionSpec as P

TP = ("tp_0", "tp_1")
FS = ("fs_0", "fs_1")
NZ, NY, NX, NC = 16, 4, 4, 2
NTP = NX * NC
ROWS = 32
COLS = 256
HEAD = 128
WIDTH = 2048
REACH = 4
ORDER = (8, 7, 9, 6, 10, 5, 11, 4, 12, 3, 13, 2, 14, 1, 15)
UP, DOWN = (8, 7, 6), (9, 10)
DIRECT = (1, 15, 2, 14, 3, 13, 4, 12, 5, 11)
NEAR = (1, 15, 2, 14, 3, 13)
FAR = (5, 11, 6, 10, 7, 9, 8)

epsilon = 1e-06
decay_rate = 0.9
learn_rate = 0.01
output_scale = 0.2

BF = jnp.bfloat16
F32 = jnp.float32


def rows_of(z, y):
    return pl.ds(pl.multiple_of(z * (NY * ROWS) + y * ROWS, ROWS), ROWS)


def around(position, step, size):
    return lax.rem(position + (step % size), size)


def send(src, dst, send_sem, recv_sem, device):
    return pltpu.make_async_remote_copy(
        src_ref=src,
        dst_ref=dst,
        send_sem=send_sem,
        recv_sem=recv_sem,
        device_id=device,
        device_id_type=pl.DeviceIdType.MESH,
    )


class Spread:
    def __init__(self, buf, sems, at, slow=()):
        self.buf = buf
        self.zs, self.zr, self.ys, self.yr, self.ya = sems
        self.at = at
        self.slow = slow

    def block(self, step):
        z, y, x, c = self.at
        return self.buf.at[rows_of(around(z, -step, NZ), y)]

    def launch(self, step, reaches, down):
        z, y, x, c = self.at
        block = self.block(step)
        for reach in reaches:
            there = around(z, -reach if down else reach, NZ)
            arrives = (step - reach if down else step + reach) % NZ
            send(block, block, self.zs, self.zr.at[arrives], (there, y, x, c)).start()

    def begin(self):
        for reach in (1, 4, 2, 3):
            self.launch(0, (reach,), False)
            self.launch(0, (reach,), True)

    def wait(self, step):
        block = self.block(step)
        send(block, block, self.zs, self.zr.at[step], self.at).wait_recv()

    def relay(self):
        for reach in (1, 2, 3, 4):
            self.launch(4, (reach,), False)
            if reach < 4:
                self.launch(12, (reach,), True)

    def to_y(self, block, far, sem):
        z, y, x, c = self.at
        send(block, block, self.ys, sem, (z, around(y, far, NY), x, c)).start()

    def across(self, step):
        block = self.block(step)
        if step in self.slow:
            onward = 3 if step % 2 else 1
            self.to_y(block, onward, self.ya.at[step])
            self.to_y(block, NY - onward, self.yr)
        else:
            for far in (2, 1, 3):
                self.to_y(block, far, self.yr)

    def onward(self, step):
        z, y, x, c = self.at
        far = 3 if step % 2 else 1
        block = self.buf.at[rows_of(around(z, -step, NZ), around(y, -far, NY))]
        send(block, block, self.ys, self.ya.at[step], self.at).wait_recv()
        self.to_y(block, far, self.yr)

    def wait_across(self):
        every = self.buf.at[pl.ds(0, (NZ * (NY - 1) - len(self.slow)) * ROWS)]
        send(every, every, self.ys, self.yr, self.at).wait_recv()

    def drain(self):
        every = self.buf.at[pl.ds(0, NZ * (NY - 1) * ROWS)]
        send(every, every, self.ys, self.yr, self.at).wait_send()
        every = self.buf.at[pl.ds(0, (NZ - 1) * ROWS)]
        send(every, every, self.zs, self.zr.at[0], self.at).wait_send()


def kernel(
    cot_hbm,
    first_hbm,
    second_hbm,
    gain_hbm,
    weight_hbm,
    left_stat_hbm,
    right_stat_hbm,
    left_root_hbm,
    right_root_hbm,
    lam_hbm,
    update_step,
    new_weight,
    new_copy,
    new_left_stat,
    new_right_stat,
    cot,
    first,
    second,
    gain,
    weight,
    left_stat,
    right_stat,
    left_root,
    right_root,
    lam,
    load_sem,
    head_out,
    partial,
    partial_half,
    from_y,
    to_z,
    from_up,
    from_down,
    from_z,
    held_weight,
    portion,
    held_step,
    stat_out,
    stat_in,
    scal_s,
    scal_z,
    rys,
    ryr,
    rzs,
    rzr,
    rup,
    rdown,
    wzs,
    wzr,
    wys,
    wyr,
    wya,
    gzs,
    gzr,
    gys,
    gyr,
    pzs,
    pzr,
    pys,
    pyr,
    sss,
    ssr,
    szs,
    szr,
    lts,
    ltr,
):
    z, y, x, c = (lax.axis_index(a) for a in ("fs_0", "fs_1", "tp_0", "tp_1"))
    at = (z, y, x, c)
    me = x * NC + c

    def z_device(step):
        return (around(z, step, NZ), y, x, c)

    def y_device(step):
        return (z, around(y, step, NY), x, c)

    def t_index(step):
        return around(me, step, NTP)

    def plane_device(up, step):
        other = t_index(step)
        return (z, around(y, up, NY), other // NC, lax.rem(other, NC))

    loads = [
        pltpu.make_async_copy(source, there, load_sem.at[k])
        for k, (source, there) in enumerate(
            (
                (first_hbm, first),
                (second_hbm, second),
                (gain_hbm, gain),
                (lam_hbm, lam),
                (cot_hbm, cot),
                (weight_hbm, weight),
                (left_root_hbm, left_root),
                (right_root_hbm, right_root),
                (left_stat_hbm, left_stat),
                (right_stat_hbm, right_stat),
            )
        )
    ]
    for load in loads:
        load.start()
    barrier = pltpu.get_barrier_semaphore()
    plane = [(up, step) for up in range(NY) for step in range(NTP) if up or step]
    peers = [z_device(s) for s in DIRECT] + [y_device(s) for s in range(1, NY)]
    peers += [plane_device(0, s) for s in range(1, NTP)]
    for peer in peers:
        pl.semaphore_signal(barrier, inc=1, device_id=peer, device_id_type=pl.DeviceIdType.MESH)

    for load in loads[:4]:
        load.wait()
    for h in range(COLS // HEAD):
        lanes = slice(h * HEAD, (h + 1) * HEAD)
        difference = first[:, lanes].astype(F32) - lam[h] * second[:, lanes].astype(F32)
        mean = jnp.mean(difference * difference, axis=-1, keepdims=True)
        scaled = difference * lax.rsqrt(mean + epsilon) * gain[...] * output_scale
        head_out[:, lanes] = scaled.astype(BF)

    def chunk(step):
        zz = around(z, step, NZ)
        rows = pl.ds(pl.multiple_of(zz * HEAD, HEAD), HEAD)
        block = lax.dot_general(
            cot[:, rows], head_out[...], (((0,), (0,)), ((), ())), preferred_element_type=F32
        )
        partial[rows] = block
        partial_half[rows] = block.astype(BF)

    def chunk_out(step):
        zz = around(z, step, NZ)
        for far in (2, 1, 3):
            send(
                partial_half.at[rows_of(zz, around(y, far, NY))],
                from_y.at[step, far - 1],
                rys,
                ryr.at[step],
                y_device(far),
            ).start()

    loads[4].wait()
    for step in ORDER[:7]:
        chunk(step)
    loads[5].wait()
    held_weight[rows_of(z, y)] = weight[...].astype(BF)

    pl.semaphore_wait(barrier, len(peers))

    for step in ORDER[:7]:
        chunk_out(step)
    weights = Spread(held_weight, (wzs, wzr, wys, wyr, wya), at, range(NZ))
    weights.begin()
    for step in (*ORDER[7:], 0):
        chunk(step)
        chunk_out(step)

    def summed(step):
        every = from_y.at[step]
        send(every, every, rys, ryr.at[step], at).wait_recv()
        total = partial[rows_of(around(z, step, NZ), y)]
        for far in range(NY - 1):
            total = total + from_y[step, far].astype(F32)
        return total

    slot = {step: k for k, step in enumerate(DIRECT)}
    for step in ORDER:
        if step in (4, 12):
            continue
        to_z[step - 1] = summed(step).astype(BF)
        if step in UP:
            copy = send(to_z.at[step - 1], from_up.at[UP.index(step)], rzs, rup, z_device(step - REACH))
        elif step in DOWN:
            copy = send(to_z.at[step - 1], from_down.at[DOWN.index(step)], rzs, rdown, z_device(step + REACH))
        else:
            copy = send(to_z.at[step - 1], from_z.at[slot[step]], rzs, rzr, z_device(step))
        copy.start()
        if step == 13:
            for far, given, sem in ((4, from_up, rup), (12, from_down, rdown)):
                total = summed(far)
                send(given, given, rzs, sem, at).wait_recv()
                for k in range(given.shape[0]):
                    total = total + given[k].astype(F32)
                to_z[far - 1] = total.astype(BF)
                send(to_z.at[far - 1], from_z.at[slot[far]], rzs, rzr, z_device(far)).start()
    own = summed(0)
    weights.across(0)
    for step in (*NEAR, 4, 12):
        weights.wait(step)
    weights.relay()
    for step in (*NEAR, 4, 12):
        weights.across(step)
    for load in loads[6:]:
        load.wait()
    send(from_z, from_z, rzs, rzr, at).wait_recv()
    for k in range(len(DIRECT)):
        own = own + from_z[k].astype(F32)

    own_half = own.astype(BF)
    portion[rows_of(z, y)] = own_half
    grads = Spread(portion, (gzs, gzr, gys, gyr, None), at)
    grads.begin()
    grads.across(0)
    grad_square = jnp.sum(own * own, axis=(0, 1), keepdims=True)
    for step in NEAR:
        grads.wait(step)
        grads.across(step)
    grads.wait(4)
    grads.wait(12)
    grads.relay()
    grads.across(4)
    grads.across(12)
    for step in FAR:
        weights.wait(step)
        weights.across(step)
    for step in FAR:
        grads.wait(step)
        grads.across(step)
    grads.wait_across()

    left_half = jnp.dot(left_root[...], portion[...], preferred_element_type=F32).astype(BF)
    steps = [
        jnp.dot(left_half[:, h * HEAD : (h + 1) * HEAD], right_root[h], preferred_element_type=F32)
        for h in range(COLS // HEAD)
    ]
    precond = jnp.concatenate(steps, axis=1)
    held_step[rows_of(z, y)] = precond.astype(BF)
    places = Spread(held_step, (pzs, pzr, pys, pyr, None), at)
    step_square = jnp.sum(precond * precond, axis=(0, 1), keepdims=True)
    low = lax.broadcasted_iota(jnp.int32, (1, HEAD), 1) < HEAD // 2
    scal_z[z] = jnp.where(low, step_square, grad_square)
    places.begin()
    for step in ORDER:
        send(scal_z.at[z], scal_z.at[z], szs, szr, z_device(step)).start()
    places.across(0)
    for j in range(NTP):
        stat_out[j] = lax.dot_general(
            own_half,
            portion[j * COLS : (j + 1) * COLS],
            (((1,), (1,)), ((), ())),
            preferred_element_type=F32,
        )
    for far in range(1, NTP):
        send(stat_out.at[t_index(far)], stat_in.at[far - 1], lts, ltr, plane_device(0, far)).start()
    for h in range(COLS // HEAD):
        lanes = slice(h * HEAD, (h + 1) * HEAD)
        product = lax.dot_general(
            portion[:, lanes], portion[:, lanes], (((0,), (0,)), ((), ())), preferred_element_type=F32
        )
        new_right_stat[h] = decay_rate * right_stat[h] + (1.0 - decay_rate) / WIDTH * product

    for step in range(NZ):
        weights.onward(step)
    for step in NEAR:
        places.wait(step)
        places.across(step)
    places.wait(4)
    places.wait(12)
    places.relay()
    places.across(4)
    places.across(12)
    send(stat_in, stat_in, lts, ltr, at).wait_recv()
    stat = stat_out[me]
    for far in range(NTP - 1):
        stat = stat + stat_in[far]
    new_left_stat[...] = decay_rate * left_stat[...] + (1.0 - decay_rate) / WIDTH * stat
    for step in FAR[:2]:
        places.wait(step)
        places.across(step)
    every = scal_z.at[pl.ds(0, NZ - 1)]
    send(every, every, szs, szr, at).wait_recv()
    total = scal_z[0]
    for k in range(1, NZ):
        total = total + scal_z[k]
    mine = y * NTP + me
    scal_s[mine] = total
    for up, step in plane:
        send(scal_s.at[mine], scal_s.at[mine], sss, ssr, plane_device(up, step)).start()
    for step in FAR[2:]:
        places.wait(step)
        places.across(step)
    every = scal_s.at[pl.ds(0, NY * NTP - 1)]
    send(every, every, sss, ssr, at).wait_recv()
    total = scal_s[0]
    for k in range(1, NY * NTP):
        total = total + scal_s[k]
    factor = jnp.sqrt((total[:, HEAD // 2 : HEAD // 2 + 1] + epsilon) / (total[:, 0:1] + epsilon))

    step_own = factor * precond
    update_step[...] = step_own
    new_weight[...] = weight[...] - learn_rate * step_own
    weights.wait_across()
    places.wait_across()
    scale = learn_rate * factor
    for k in range(NZ):
        rows = pl.ds(k * HEAD, HEAD)
        new_copy[rows] = (held_weight[rows].astype(F32) - scale * held_step[rows].astype(F32)).astype(BF)

    every = partial_half.at[pl.ds(0, NZ * (NY - 1) * ROWS)]
    send(every, every, rys, ryr.at[0], at).wait_send()
    send(to_z, to_z, rzs, rzr, at).wait_send()
    every = scal_s.at[pl.ds(0, NY * NTP - 1)]
    send(every, every, sss, ssr, at).wait_send()
    every = scal_z.at[pl.ds(0, NZ - 1)]
    send(every, every, szs, szr, at).wait_send()
    send(stat_in, stat_in, lts, ltr, at).wait_send()
    for spread in (weights, grads, places):
        spread.drain()


def store(*refs):
    given, out, sem = refs[:5], refs[5:10], refs[10]
    copies = [pltpu.make_async_copy(a, b, sem.at[k]) for k, (a, b) in enumerate(zip(given, out))]
    for copy in copies:
        copy.start()
    for copy in copies:
        copy.wait()


def shards(
    cotangent,
    values_first,
    values_second,
    head_lambda,
    out_gain,
    weight,
    left_stat,
    right_stat,
    left_root,
    right_root,
):
    vmem = pl.BlockSpec(memory_space=pltpu.VMEM)
    anywhere = pl.BlockSpec(memory_space=pl.ANY)
    dma = pltpu.SemaphoreType.DMA
    spread = [dma, dma((NZ,)), dma, dma]
    given = (
        cotangent,
        values_first,
        values_second,
        out_gain.reshape(1, HEAD),
        weight,
        left_stat,
        right_stat,
        left_root,
        right_root,
        head_lambda,
    )
    results = (
        jax.ShapeDtypeStruct((ROWS, COLS), F32),
        jax.ShapeDtypeStruct((ROWS, COLS), F32),
        jax.ShapeDtypeStruct((WIDTH, COLS), BF),
        jax.ShapeDtypeStruct((ROWS, COLS), F32),
        jax.ShapeDtypeStruct((COLS // HEAD, HEAD, HEAD), F32),
    )
    outs = pl.pallas_call(
        kernel,
        out_shape=results,
        in_specs=[pl.BlockSpec(memory_space=pltpu.HBM)] * 10,
        out_specs=[vmem] * 5,
        scratch_shapes=[
            *[pltpu.VMEM(a.shape, a.dtype) for a in given[:9]],
            pltpu.SMEM(head_lambda.shape, F32),
            dma((10,)),
            pltpu.VMEM((128, COLS), BF),
            pltpu.VMEM((WIDTH, COLS), F32),
            pltpu.VMEM((WIDTH, COLS), BF),
            pltpu.VMEM((NZ, NY - 1, ROWS, COLS), BF),
            pltpu.VMEM((NZ - 1, ROWS, COLS), BF),
            pltpu.VMEM((len(UP), ROWS, COLS), BF),
            pltpu.VMEM((len(DOWN), ROWS, COLS), BF),
            pltpu.VMEM((len(DIRECT), ROWS, COLS), BF),
            pltpu.VMEM((WIDTH, COLS), BF),
            pltpu.VMEM((WIDTH, COLS), BF),
            pltpu.VMEM((WIDTH, COLS), BF),
            pltpu.VMEM((NTP, ROWS, COLS), F32),
            pltpu.VMEM((NTP - 1, ROWS, COLS), F32),
            pltpu.VMEM((NY * NTP, 1, HEAD), F32),
            pltpu.VMEM((NZ, 1, HEAD), F32),
            dma,
            dma((NZ,)),
            dma,
            dma,
            dma,
            dma,
            *spread,
            dma((NZ,)),
            *spread,
            *spread,
            dma,
            dma,
            dma,
            dma,
            dma,
            dma,
        ],
        compiler_params=pltpu.CompilerParams(
            collective_id=0, has_side_effects=True, vmem_limit_bytes=28 * 2**20
        ),
        name="fused",
    )(*[pltpu.with_memory_space_constraint(a, pltpu.HBM) for a in given])
    return pl.pallas_call(
        store,
        out_shape=results,
        in_specs=[vmem] * 5,
        out_specs=[anywhere] * 5,
        scratch_shapes=[dma((5,))],
        compiler_params=pltpu.CompilerParams(vmem_limit_bytes=8 * 2**20),
        name="store",
    )(*outs)


def solution(mesh):
    finer = Mesh(mesh.devices.reshape(NZ, NY, NX, NC), ("fs_0", "fs_1", "tp_0", "tp_1"))
    in_specs = (
        P(FS, None),
        P(FS, TP),
        P(FS, TP),
        P(TP),
        P(),
        P(FS, TP),
        P(FS, TP),
        P(TP, None, None),
        P(FS, None),
        P(TP, None, None),
    )
    out_specs = (P(FS, TP), P(FS, TP), P(None, TP), P(FS, TP), P(TP, None, None))
    return jax.shard_map(
        shards, mesh=finer, in_specs=in_specs, out_specs=out_specs, check_vma=False
    )
```

```python
import jax
import jax.numpy as jnp
from jax import lax
from jax.experimental import pallas as pl
from jax.experimental.pallas import tpu as pltpu
from jax.sharding import Mesh
from jax.sharding import PartitionSpec as P

TP = ("tp_0", "tp_1")
FS = ("fs_0", "fs_1")
NZ, NY, NX, NC = 16, 4, 4, 2
NTP = NX * NC
ROWS = 32
COLS = 256
HEAD = 128
WIDTH = 2048
REACH = 4
HEADS = COLS // HEAD
ORDER = (8, 7, 9, 6, 10, 5, 11, 4, 12, 3, 13, 2, 14, 1, 15, 0)
BATCH = ((8, 7), (9, 6), (10,), (5, 11), (4, 12), (3, 13), (2, 14), (1, 15), (0,))
UP, DOWN = (8, 7, 6), (9, 10)
DIRECT = (1, 15, 2, 14, 3, 13, 4, 12, 5, 11)
NEAR = ((1, 15), (2, 14), (3, 13))
MID = ((4,), (12,))
FAR = ((5, 11), (6, 10), (7, 9), (8,))
GROUPS = NEAR + MID + FAR
GROUP_OF = {step: k for k, group in enumerate(GROUPS) for step in group}

epsilon = 1e-06
decay_rate = 0.9
learn_rate = 0.01
output_scale = 0.2

BF = jnp.bfloat16
F32 = jnp.float32


def rows_of(z, y):
    return pl.ds(pl.multiple_of(z * (NY * ROWS) + y * ROWS, ROWS), ROWS)


def around(position, step, size):
    return lax.rem(position + (step % size), size)


def send(src, dst, send_sem, recv_sem, device):
    return pltpu.make_async_remote_copy(
        src_ref=src,
        dst_ref=dst,
        send_sem=send_sem,
        recv_sem=recv_sem,
        device_id=device,
        device_id_type=pl.DeviceIdType.MESH,
    )


class Spread:
    def __init__(self, buf, sems, at, slow=False):
        self.buf = buf
        self.zs, self.zr, self.ys, self.yr, self.ya = sems
        self.at = at
        self.slow = slow

    def block(self, step):
        z, y, x, c = self.at
        return self.buf.at[rows_of(around(z, -step, NZ), y)]

    def whole(self, blocks):
        return self.buf.at[pl.ds(0, blocks * ROWS)]

    def launch(self, step, reach, down):
        z, y, x, c = self.at
        block = self.block(step)
        there = around(z, -reach if down else reach, NZ)
        arrives = (step - reach if down else step + reach) % NZ
        send(block, block, self.zs, self.zr.at[GROUP_OF[arrives]], (there, y, x, c)).start()

    def begin(self):
        for reach in (1, 4, 2, 3):
            self.launch(0, reach, False)
            self.launch(0, reach, True)

    def wait(self, group):
        every = self.whole(len(group))
        send(every, every, self.zs, self.zr.at[GROUP_OF[group[0]]], self.at).wait_recv()

    def relay(self):
        for reach in (1, 2, 3, 4):
            self.launch(4, reach, False)
            if reach < 4:
                self.launch(12, reach, True)

    def to_y(self, block, far, sem):
        z, y, x, c = self.at
        send(block, block, self.ys, sem, (z, around(y, far, NY), x, c)).start()

    def across(self, group):
        for step in group:
            block = self.block(step)
            if self.slow:
                onward = 3 if step % 2 else 1
                self.to_y(block, onward, self.ya)
                self.to_y(block, NY - onward, self.yr)
            else:
                for far in (2, 1, 3):
                    self.to_y(block, far, self.yr)

    def take(self, groups):
        for group in groups:
            self.wait(group)
            self.across(group)

    def onward(self):
        z, y, x, c = self.at
        every = self.whole(NZ)
        send(every, every, self.ys, self.ya, self.at).wait_recv()
        for step in range(NZ):
            far = 3 if step % 2 else 1
            block = self.buf.at[rows_of(around(z, -step, NZ), around(y, -far, NY))]
            self.to_y(block, far, self.yr)

    def wait_across(self):
        every = self.whole(NZ * (2 if self.slow else 3))
        send(every, every, self.ys, self.yr, self.at).wait_recv()

    def drain(self):
        every = self.whole(NZ * (NY - 1))
        send(every, every, self.ys, self.yr, self.at).wait_send()
        every = self.whole(NZ - 1)
        send(every, every, self.zs, self.zr.at[0], self.at).wait_send()


def kernel(*refs):
    refs = list(refs)

    def grab(count):
        taken = refs[:count]
        del refs[:count]
        return taken

    sources = grab(10)
    update_step, new_weight, new_copy, new_left_stat, new_right_stat = grab(5)
    local = grab(10)
    first, second, gain, lam, cot, weight, left_root, right_root, left_stat, right_stat = local
    (load_sem,) = grab(1)
    head_out, partial = grab(2)
    partial_half, from_y, to_z, from_up, from_down, from_z = (grab(HEADS) for _ in range(6))
    (held_weight,) = grab(1)
    portion, held_step = grab(HEADS), grab(HEADS)
    stat_out, stat_in, scal_s, scal_z = grab(4)
    rys, ryr, rzs, rzr, rup, rdown = (grab(HEADS) for _ in range(6))
    wsems = grab(5)
    gsems = [[*grab(4), None] for _ in range(HEADS)]
    psems = [[*grab(4), None] for _ in range(HEADS)]
    sss, ssr, szs, szr, lts, ltr = grab(6)

    z, y, x, c = (lax.axis_index(a) for a in ("fs_0", "fs_1", "tp_0", "tp_1"))
    at = (z, y, x, c)
    me = x * NC + c
    both = range(HEADS)
    lanes = [slice(h * HEAD, (h + 1) * HEAD) for h in both]

    def z_device(step):
        return (around(z, step, NZ), y, x, c)

    def y_device(step):
        return (z, around(y, step, NY), x, c)

    def t_index(step):
        return around(me, step, NTP)

    def t_device(step):
        other = t_index(step)
        return (z, y, other // NC, lax.rem(other, NC))

    loads = [pltpu.make_async_copy(a, b, load_sem.at[k]) for k, (a, b) in enumerate(zip(sources, local))]
    for load in loads:
        load.start()
    barrier = pltpu.get_barrier_semaphore()
    peers = [z_device(s) for s in DIRECT] + [y_device(s) for s in range(1, NY)]
    peers += [t_device(s) for s in range(1, NTP)]
    for peer in peers:
        pl.semaphore_signal(barrier, inc=1, device_id=peer, device_id_type=pl.DeviceIdType.MESH)

    for load in loads[:4]:
        load.wait()
    for h in both:
        difference = first[:, lanes[h]].astype(F32) - lam[h] * second[:, lanes[h]].astype(F32)
        mean = jnp.mean(difference * difference, axis=-1, keepdims=True)
        scaled = difference * lax.rsqrt(mean + epsilon) * gain[...] * output_scale
        head_out[:, lanes[h]] = scaled.astype(BF)

    def chunk(step):
        zz = around(z, step, NZ)
        rows = pl.ds(pl.multiple_of(zz * HEAD, HEAD), HEAD)
        block = lax.dot_general(
            cot[:, rows], head_out[...], (((0,), (0,)), ((), ())), preferred_element_type=F32
        )
        partial[rows] = block
        for h in both:
            partial_half[h][rows] = block[:, lanes[h]].astype(BF)

    batch_of = {step: k for k, group in enumerate(BATCH) for step in group}
    spot = {step: k for k, step in enumerate(step for group in BATCH for step in group)}

    def chunk_out(h, step):
        zz = around(z, step, NZ)
        for far in (2, 1, 3):
            send(
                partial_half[h].at[rows_of(zz, around(y, far, NY))],
                from_y[h].at[spot[step], far - 1],
                rys[h],
                ryr[h].at[batch_of[step]],
                y_device(far),
            ).start()

    loads[4].wait()
    for step in ORDER[:7]:
        chunk(step)
    loads[5].wait()
    held_weight[rows_of(z, y)] = weight[...].astype(BF)

    pl.semaphore_wait(barrier, len(peers))

    for h in both:
        for step in ORDER[:5]:
            chunk_out(h, step)
    weights = Spread(held_weight, wsems, at, True)
    weights.begin()
    for step in ORDER[5:7]:
        chunk_out(0, step)
    for step in ORDER[7:]:
        chunk(step)
        chunk_out(0, step)
    for step in ORDER[5:]:
        chunk_out(1, step)

    def arrive(h, group):
        block = from_y[h].at[pl.ds(spot[group[0]], len(group))]
        send(block, block, rys[h], ryr[h].at[batch_of[group[0]]], at).wait_recv()

    def summed(h, step):
        total = partial[rows_of(around(z, step, NZ), y), lanes[h]]
        for far in range(NY - 1):
            total = total + from_y[h][spot[step], far].astype(F32)
        return total

    slot = {step: k for k, step in enumerate(DIRECT)}

    def pass_on(h, groups):
        for group in groups:
            arrive(h, group)
            for step in group:
                out = to_z[h].at[step - 1]
                to_z[h][step - 1] = summed(h, step).astype(BF)
                if step in UP:
                    send(out, from_up[h].at[UP.index(step)], rzs[h], rup[h], z_device(step - REACH)).start()
                elif step in DOWN:
                    send(out, from_down[h].at[DOWN.index(step)], rzs[h], rdown[h], z_device(step + REACH)).start()
                else:
                    send(out, from_z[h].at[slot[step]], rzs[h], rzr[h], z_device(step)).start()

    def combine(h):
        arrive(h, BATCH[4])
        for far, given, sem in ((4, from_up[h], rup[h]), (12, from_down[h], rdown[h])):
            total = summed(h, far)
            send(given, given, rzs[h], sem, at).wait_recv()
            for k in range(given.shape[0]):
                total = total + given[k].astype(F32)
            to_z[h][far - 1] = total.astype(BF)
            send(to_z[h].at[far - 1], from_z[h].at[slot[far]], rzs[h], rzr[h], z_device(far)).start()

    def finish(h):
        arrive(h, BATCH[8])
        own = summed(h, 0)
        send(from_z[h], from_z[h], rzs[h], rzr[h], at).wait_recv()
        for k in range(len(DIRECT)):
            own = own + from_z[h][k].astype(F32)
        return own

    pass_on(0, BATCH[:3])
    pass_on(1, BATCH[:3])
    pass_on(0, BATCH[3:4])
    combine(0)
    pass_on(0, BATCH[5:8])
    pass_on(1, BATCH[3:4])
    combine(1)
    pass_on(1, BATCH[5:8])
    own, own_half, grads = [None] * HEADS, [None] * HEADS, [None] * HEADS

    def gather(h):
        own[h] = finish(h)
        own_half[h] = own[h].astype(BF)
        portion[h][rows_of(z, y)] = own_half[h]
        grads[h] = Spread(portion[h], gsems[h], at)
        grads[h].begin()
        grads[h].across((0,))

    gather(0)
    weights.across((0,))
    for group in NEAR + MID:
        weights.wait(group)
    for group in NEAR + MID:
        weights.across(group)
    for load in loads[6:]:
        load.wait()
    gather(1)
    grads[0].take(NEAR)
    for group in MID:
        grads[0].wait(group)
    grads[0].relay()
    for group in MID:
        grads[0].across(group)
    grads[1].take(NEAR)
    for group in MID:
        grads[1].wait(group)
    grads[1].relay()
    weights.relay()
    for group in MID:
        grads[1].across(group)
    grads[0].take(FAR)
    grads[1].take(FAR)

    precond, places = [None] * HEADS, [None] * HEADS

    def advance(h):
        left_half = jnp.dot(left_root[...], portion[h][...], preferred_element_type=F32).astype(BF)
        precond[h] = jnp.dot(left_half, right_root[h], preferred_element_type=F32)
        held_step[h][rows_of(z, y)] = precond[h].astype(BF)
        places[h] = Spread(held_step[h], psems[h], at)
        places[h].begin()
        places[h].across((0,))

    grads[0].wait_across()
    advance(0)
    weights.take(FAR)
    grads[1].wait_across()
    advance(1)
    squares = [jnp.sum(v * v, axis=(0, 1), keepdims=True) for v in (*precond, *own)]
    low = lax.broadcasted_iota(jnp.int32, (1, HEAD), 1) < HEAD // 2
    mine = z * NY + y
    scal_z[mine] = jnp.where(low, squares[0] + squares[1], squares[2] + squares[3])
    for step in ORDER:
        for up in (2, 1, 3, 0):
            if step or up:
                there = (around(z, step, NZ), around(y, up, NY), x, c)
                send(scal_z.at[mine], scal_z.at[mine], szs, szr, there).start()
    places[0].take(NEAR)
    for group in MID:
        places[0].wait(group)
    places[0].relay()
    for group in MID:
        places[0].across(group)

    contract = (((1,), (1,)), ((), ()))
    for j in range(NTP):
        rows = slice(j * COLS, (j + 1) * COLS)
        stat_out[j] = sum(
            lax.dot_general(own_half[h], portion[h][rows], contract, preferred_element_type=F32)
            for h in both
        )
    for far in range(1, NTP):
        send(stat_out.at[t_index(far)], stat_in.at[far - 1], lts, ltr, t_device(far)).start()
    for h in both:
        product = lax.dot_general(
            portion[h][...], portion[h][...], (((0,), (0,)), ((), ())), preferred_element_type=F32
        )
        new_right_stat[h] = decay_rate * right_stat[h] + (1.0 - decay_rate) / WIDTH * product
    weights.onward()
    places[1].take(NEAR)
    for group in MID:
        places[1].wait(group)
    places[1].relay()
    for group in MID:
        places[1].across(group)
    places[0].take(FAR)
    every = scal_z.at[pl.ds(0, NZ * NY - 1)]
    send(every, every, szs, szr, at).wait_recv()
    total = scal_z[0]
    for k in range(1, NZ * NY):
        total = total + scal_z[k]
    scal_s[me] = total
    for step in range(1, NTP):
        send(scal_s.at[me], scal_s.at[me], sss, ssr, t_device(step)).start()
    places[1].take(FAR)
    send(stat_in, stat_in, lts, ltr, at).wait_recv()
    stat = stat_out[me]
    for far in range(NTP - 1):
        stat = stat + stat_in[far]
    new_left_stat[...] = decay_rate * left_stat[...] + (1.0 - decay_rate) / WIDTH * stat
    every = scal_s.at[pl.ds(0, NTP - 1)]
    send(every, every, sss, ssr, at).wait_recv()
    total = scal_s[0]
    for k in range(1, NTP):
        total = total + scal_s[k]
    factor = jnp.sqrt((total[:, HEAD // 2 : HEAD // 2 + 1] + epsilon) / (total[:, 0:1] + epsilon))
    for h in both:
        step_own = factor * precond[h]
        update_step[:, lanes[h]] = step_own
        new_weight[:, lanes[h]] = weight[:, lanes[h]] - learn_rate * step_own
    weights.wait_across()
    scale = learn_rate * factor
    for h in both:
        places[h].wait_across()
        for k in range(NZ):
            rows = pl.ds(k * HEAD, HEAD)
            held = held_weight[rows, lanes[h]].astype(F32)
            new_copy[rows, lanes[h]] = (held - scale * held_step[h][rows].astype(F32)).astype(BF)

    for h in both:
        every = partial_half[h].at[pl.ds(0, NZ * (NY - 1) * ROWS)]
        send(every, every, rys[h], ryr[h].at[0], at).wait_send()
        send(to_z[h], to_z[h], rzs[h], rzr[h], at).wait_send()
    every = scal_s.at[pl.ds(0, NTP - 1)]
    send(every, every, sss, ssr, at).wait_send()
    every = scal_z.at[pl.ds(0, NZ * NY - 1)]
    send(every, every, szs, szr, at).wait_send()
    send(stat_in, stat_in, lts, ltr, at).wait_send()
    for spread in (weights, *grads, *places):
        spread.drain()


def store(*refs):
    given, out, sem = refs[:5], refs[5:10], refs[10]
    copies = [pltpu.make_async_copy(a, b, sem.at[k]) for k, (a, b) in enumerate(zip(given, out))]
    for copy in copies:
        copy.start()
    for copy in copies:
        copy.wait()


def shards(
    cotangent,
    values_first,
    values_second,
    head_lambda,
    out_gain,
    weight,
    left_stat,
    right_stat,
    left_root,
    right_root,
):
    vmem = pl.BlockSpec(memory_space=pltpu.VMEM)
    anywhere = pl.BlockSpec(memory_space=pl.ANY)
    dma = pltpu.SemaphoreType.DMA
    spread = [dma, dma((len(GROUPS),)), dma, dma]
    given = (
        values_first,
        values_second,
        out_gain.reshape(1, HEAD),
        head_lambda,
        cotangent,
        weight,
        left_root,
        right_root,
        left_stat,
        right_stat,
    )
    local = [pltpu.SMEM(a.shape, F32) if a is head_lambda else pltpu.VMEM(a.shape, a.dtype) for a in given]

    def per_head(*shape):
        return [pltpu.VMEM((*shape, HEAD), BF)] * HEADS

    results = (
        jax.ShapeDtypeStruct((ROWS, COLS), F32),
        jax.ShapeDtypeStruct((ROWS, COLS), F32),
        jax.ShapeDtypeStruct((WIDTH, COLS), BF),
        jax.ShapeDtypeStruct((ROWS, COLS), F32),
        jax.ShapeDtypeStruct((COLS // HEAD, HEAD, HEAD), F32),
    )
    outs = pl.pallas_call(
        kernel,
        out_shape=results,
        in_specs=[pl.BlockSpec(memory_space=pltpu.HBM)] * 10,
        out_specs=[vmem] * 5,
        scratch_shapes=[
            *local,
            dma((10,)),
            pltpu.VMEM((128, COLS), BF),
            pltpu.VMEM((WIDTH, COLS), F32),
            *per_head(WIDTH),
            *per_head(NZ, NY - 1, ROWS),
            *per_head(NZ - 1, ROWS),
            *per_head(len(UP), ROWS),
            *per_head(len(DOWN), ROWS),
            *per_head(len(DIRECT), ROWS),
            pltpu.VMEM((WIDTH, COLS), BF),
            *per_head(WIDTH),
            *per_head(WIDTH),
            pltpu.VMEM((NTP, ROWS, COLS), F32),
            pltpu.VMEM((NTP - 1, ROWS, COLS), F32),
            pltpu.VMEM((NTP, 1, HEAD), F32),
            pltpu.VMEM((NZ * NY, 1, HEAD), F32),
            *[dma] * HEADS,
            *[dma((len(BATCH),))] * HEADS,
            *[dma] * (4 * HEADS),
            *spread,
            dma,
            *spread * (2 * HEADS),
            *[dma] * 6,
        ],
        compiler_params=pltpu.CompilerParams(
            collective_id=0, has_side_effects=True, vmem_limit_bytes=28 * 2**20
        ),
        name="fused",
    )(*[pltpu.with_memory_space_constraint(a, pltpu.HBM) for a in given])
    return pl.pallas_call(
        store,
        out_shape=results,
        in_specs=[vmem] * 5,
        out_specs=[anywhere] * 5,
        scratch_shapes=[dma((5,))],
        compiler_params=pltpu.CompilerParams(vmem_limit_bytes=8 * 2**20),
        name="store",
    )(*outs)


def solution(mesh):
    finer = Mesh(mesh.devices.reshape(NZ, NY, NX, NC), ("fs_0", "fs_1", "tp_0", "tp_1"))
    in_specs = (
        P(FS, None),
        P(FS, TP),
        P(FS, TP),
        P(TP),
        P(),
        P(FS, TP),
        P(FS, TP),
        P(TP, None, None),
        P(FS, None),
        P(TP, None, None),
    )
    out_specs = (P(FS, TP), P(FS, TP), P(None, TP), P(FS, TP), P(TP, None, None))
    return jax.shard_map(
        shards, mesh=finer, in_specs=in_specs, out_specs=out_specs, check_vma=False
    )
```

```python
import jax
import jax.numpy as jnp
from jax import lax
from jax.experimental import pallas as pl
from jax.experimental.pallas import tpu as pltpu
from jax.sharding import Mesh
from jax.sharding import PartitionSpec as P

TP = ("tp_0", "tp_1")
FS = ("fs_0", "fs_1")
NZ, NY, NX, NC = 16, 4, 4, 2
NTP = NX * NC
ROWS = 32
COLS = 256
HEAD = 128
WIDTH = 2048
REACH = 4
HEADS = COLS // HEAD
ORDER = (8, 7, 9, 6, 10, 5, 11, 4, 12, 3, 13, 2, 14, 1, 15, 0)
BATCH = ((8, 7), (9, 6), (10,), (5, 11), (4, 12), (3, 13), (2, 14), (1, 15), (0,))
UP, DOWN = (8, 7, 6, 5), (9, 10, 11)
DIRECT = (1, 15, 2, 14, 3, 13, 4, 12)
NEAR = ((1, 15), (2, 14), (3, 13))
MID = ((4,), (12,))
FAR = ((5, 11), (6, 10), (7, 9), (8,))
GROUPS = NEAR + MID + FAR
GROUP_OF = {step: k for k, group in enumerate(GROUPS) for step in group}

epsilon = 1e-06
decay_rate = 0.9
learn_rate = 0.01
output_scale = 0.2

BF = jnp.bfloat16
F32 = jnp.float32


def rows_of(z, y):
    return pl.ds(pl.multiple_of(z * (NY * ROWS) + y * ROWS, ROWS), ROWS)


def around(position, step, size):
    return lax.rem(position + (step % size), size)


def send(src, dst, send_sem, recv_sem, device):
    return pltpu.make_async_remote_copy(
        src_ref=src,
        dst_ref=dst,
        send_sem=send_sem,
        recv_sem=recv_sem,
        device_id=device,
        device_id_type=pl.DeviceIdType.MESH,
    )


class Spread:
    def __init__(self, buf, sems, at, slow=False):
        self.buf = buf
        self.zs, self.zr, self.ys, self.yr, self.ya = sems
        self.at = at
        self.slow = slow

    def block(self, step):
        z, y, x, c = self.at
        return self.buf.at[rows_of(around(z, -step, NZ), y)]

    def whole(self, blocks):
        return self.buf.at[pl.ds(0, blocks * ROWS)]

    def launch(self, step, reach, down):
        z, y, x, c = self.at
        block = self.block(step)
        there = around(z, -reach if down else reach, NZ)
        arrives = (step - reach if down else step + reach) % NZ
        send(block, block, self.zs, self.zr.at[GROUP_OF[arrives]], (there, y, x, c)).start()

    def begin(self):
        for reach in (1, 4, 2, 3):
            self.launch(0, reach, False)
            self.launch(0, reach, True)

    def wait(self, group):
        every = self.whole(len(group))
        send(every, every, self.zs, self.zr.at[GROUP_OF[group[0]]], self.at).wait_recv()

    def relay(self):
        for reach in (1, 2, 3, 4):
            self.launch(4, reach, False)
            if reach < 4:
                self.launch(12, reach, True)

    def to_y(self, block, far, sem):
        z, y, x, c = self.at
        send(block, block, self.ys, sem, (z, around(y, far, NY), x, c)).start()

    def across(self, group):
        for step in group:
            block = self.block(step)
            if self.slow:
                onward = 3 if step % 2 else 1
                self.to_y(block, onward, self.ya)
                self.to_y(block, NY - onward, self.yr)
            else:
                for far in (2, 1, 3):
                    self.to_y(block, far, self.yr)

    def take(self, groups):
        for group in groups:
            self.wait(group)
            self.across(group)

    def onward(self):
        z, y, x, c = self.at
        every = self.whole(NZ)
        send(every, every, self.ys, self.ya, self.at).wait_recv()
        for step in range(NZ):
            far = 3 if step % 2 else 1
            block = self.buf.at[rows_of(around(z, -step, NZ), around(y, -far, NY))]
            self.to_y(block, far, self.yr)

    def wait_across(self):
        every = self.whole(NZ * (2 if self.slow else 3))
        send(every, every, self.ys, self.yr, self.at).wait_recv()

    def drain(self):
        every = self.whole(NZ * (NY - 1))
        send(every, every, self.ys, self.yr, self.at).wait_send()
        every = self.whole(NZ - 1)
        send(every, every, self.zs, self.zr.at[0], self.at).wait_send()


def kernel(*refs):
    refs = list(refs)

    def grab(count):
        taken = refs[:count]
        del refs[:count]
        return taken

    sources = grab(10)
    update_step, new_weight, new_copy, new_left_stat, new_right_stat = grab(5)
    local = grab(10)
    first, second, gain, lam, cot, weight, left_root, right_root, left_stat, right_stat = local
    (load_sem,) = grab(1)
    head_out, partial = grab(2)
    partial_half, from_y, to_z, from_up, from_down, from_z = (grab(HEADS) for _ in range(6))
    (held_weight,) = grab(1)
    portion, held_step = grab(HEADS), grab(HEADS)
    stat_out, stat_in, scal_s, scal_z = grab(4)
    rys, ryr, rzs, rzr, rup, rdown = (grab(HEADS) for _ in range(6))
    wsems = grab(5)
    gsems = [[*grab(4), None] for _ in range(HEADS)]
    psems = [[*grab(4), None] for _ in range(HEADS)]
    sss, ssr, szs, szr, lts, ltr = grab(6)

    z, y, x, c = (lax.axis_index(a) for a in ("fs_0", "fs_1", "tp_0", "tp_1"))
    at = (z, y, x, c)
    me = x * NC + c
    both = range(HEADS)
    lanes = [slice(h * HEAD, (h + 1) * HEAD) for h in both]

    def z_device(step):
        return (around(z, step, NZ), y, x, c)

    def y_device(step):
        return (z, around(y, step, NY), x, c)

    def t_index(step):
        return around(me, step, NTP)

    def t_device(step):
        other = t_index(step)
        return (z, y, other // NC, lax.rem(other, NC))

    loads = [pltpu.make_async_copy(a, b, load_sem.at[k]) for k, (a, b) in enumerate(zip(sources, local))]
    for load in loads:
        load.start()
    barrier = pltpu.get_barrier_semaphore()
    peers = [z_device(s) for s in DIRECT] + [y_device(s) for s in range(1, NY)]
    peers += [t_device(s) for s in range(1, NTP)]
    for peer in peers:
        pl.semaphore_signal(barrier, inc=1, device_id=peer, device_id_type=pl.DeviceIdType.MESH)

    for load in loads[:4]:
        load.wait()
    for h in both:
        difference = first[:, lanes[h]].astype(F32) - lam[h] * second[:, lanes[h]].astype(F32)
        mean = jnp.mean(difference * difference, axis=-1, keepdims=True)
        scaled = difference * lax.rsqrt(mean + epsilon) * gain[...] * output_scale
        head_out[:, lanes[h]] = scaled.astype(BF)

    def chunk(step):
        zz = around(z, step, NZ)
        rows = pl.ds(pl.multiple_of(zz * HEAD, HEAD), HEAD)
        block = lax.dot_general(
            cot[:, rows], head_out[...], (((0,), (0,)), ((), ())), preferred_element_type=F32
        )
        partial[rows] = block
        for h in both:
            partial_half[h][rows] = block[:, lanes[h]].astype(BF)

    batch_of = {step: k for k, group in enumerate(BATCH) for step in group}
    spot = {step: k for k, step in enumerate(step for group in BATCH for step in group)}

    def chunk_out(h, step):
        zz = around(z, step, NZ)
        for far in (2, 1, 3):
            send(
                partial_half[h].at[rows_of(zz, around(y, far, NY))],
                from_y[h].at[spot[step], far - 1],
                rys[h],
                ryr[h].at[batch_of[step]],
                y_device(far),
            ).start()

    loads[4].wait()
    for step in ORDER[:7]:
        chunk(step)
    loads[5].wait()
    held_weight[rows_of(z, y)] = weight[...].astype(BF)

    pl.semaphore_wait(barrier, len(peers))

    for h in both:
        for step in ORDER[:7]:
            chunk_out(h, step)
    weights = Spread(held_weight, wsems, at, True)
    weights.begin()
    for step in ORDER[7:]:
        chunk(step)
        chunk_out(0, step)
    for step in ORDER[7:]:
        chunk_out(1, step)

    def arrive(h, group):
        block = from_y[h].at[pl.ds(spot[group[0]], len(group))]
        send(block, block, rys[h], ryr[h].at[batch_of[group[0]]], at).wait_recv()

    def summed(h, step):
        total = partial[rows_of(around(z, step, NZ), y), lanes[h]]
        for far in range(NY - 1):
            total = total + from_y[h][spot[step], far].astype(F32)
        return total

    slot = {step: k for k, step in enumerate(DIRECT)}

    def pass_on(h, groups):
        for group in groups:
            arrive(h, group)
            for step in group:
                out = to_z[h].at[step - 1]
                to_z[h][step - 1] = summed(h, step).astype(BF)
                if step in UP:
                    send(out, from_up[h].at[UP.index(step)], rzs[h], rup[h], z_device(step - REACH)).start()
                elif step in DOWN:
                    send(out, from_down[h].at[DOWN.index(step)], rzs[h], rdown[h], z_device(step + REACH)).start()
                else:
                    send(out, from_z[h].at[slot[step]], rzs[h], rzr[h], z_device(step)).start()

    def combine(h):
        arrive(h, BATCH[4])
        for far, given, sem in ((4, from_up[h], rup[h]), (12, from_down[h], rdown[h])):
            total = summed(h, far)
            send(given, given, rzs[h], sem, at).wait_recv()
            for k in range(given.shape[0]):
                total = total + given[k].astype(F32)
            to_z[h][far - 1] = total.astype(BF)
            send(to_z[h].at[far - 1], from_z[h].at[slot[far]], rzs[h], rzr[h], z_device(far)).start()

    def finish(h):
        arrive(h, BATCH[8])
        own = summed(h, 0)
        send(from_z[h], from_z[h], rzs[h], rzr[h], at).wait_recv()
        for k in range(len(DIRECT)):
            own = own + from_z[h][k].astype(F32)
        return own

    pass_on(0, BATCH[:4])
    pass_on(1, BATCH[:4])
    combine(0)
    pass_on(0, BATCH[5:8])
    combine(1)
    pass_on(1, BATCH[5:8])
    own, own_half, grads = [None] * HEADS, [None] * HEADS, [None] * HEADS

    def gather(h):
        own[h] = finish(h)
        own_half[h] = own[h].astype(BF)
        portion[h][rows_of(z, y)] = own_half[h]
        grads[h] = Spread(portion[h], gsems[h], at)
        grads[h].begin()
        grads[h].across((0,))

    gather(0)
    weights.across((0,))
    for group in NEAR + MID:
        weights.wait(group)
    for group in NEAR + MID:
        weights.across(group)
    for load in loads[6:]:
        load.wait()
    gather(1)
    grads[0].take(NEAR)
    for group in MID:
        grads[0].wait(group)
    grads[0].relay()
    for group in MID:
        grads[0].across(group)
    grads[1].take(NEAR)
    for group in MID:
        grads[1].wait(group)
    grads[1].relay()
    weights.relay()
    for group in MID:
        grads[1].across(group)
    grads[0].take(FAR)
    grads[1].take(FAR)

    precond, places = [None] * HEADS, [None] * HEADS

    def send_squares():
        squares = [jnp.sum(v * v, axis=(0, 1), keepdims=True) for v in (*precond, *own)]
        low = lax.broadcasted_iota(jnp.int32, (1, HEAD), 1) < HEAD // 2
        mine = z * NY + y
        scal_z[mine] = jnp.where(low, squares[0] + squares[1], squares[2] + squares[3])
        for step in ORDER:
            for up in (2, 1, 3, 0):
                if step or up:
                    there = (around(z, step, NZ), around(y, up, NY), x, c)
                    send(scal_z.at[mine], scal_z.at[mine], szs, szr, there).start()

    def advance(h):
        left_half = jnp.dot(left_root[...], portion[h][...], preferred_element_type=F32).astype(BF)
        precond[h] = jnp.dot(left_half, right_root[h], preferred_element_type=F32)
        if h == HEADS - 1:
            send_squares()
        held_step[h][rows_of(z, y)] = precond[h].astype(BF)
        places[h] = Spread(held_step[h], psems[h], at)
        places[h].begin()
        places[h].across((0,))

    grads[0].wait_across()
    advance(0)
    weights.take(FAR)
    grads[1].wait_across()
    advance(1)
    places[0].take(NEAR)
    for group in MID:
        places[0].wait(group)
    places[0].relay()
    for group in MID:
        places[0].across(group)

    weights.onward()
    places[1].take(NEAR)
    for group in MID:
        places[1].wait(group)
    places[1].relay()
    for group in MID:
        places[1].across(group)
    contract = (((1,), (1,)), ((), ()))
    for j in range(NTP):
        rows = slice(j * COLS, (j + 1) * COLS)
        stat_out[j] = sum(
            lax.dot_general(own_half[h], portion[h][rows], contract, preferred_element_type=F32)
            for h in both
        )
    for far in range(1, NTP):
        send(stat_out.at[t_index(far)], stat_in.at[far - 1], lts, ltr, t_device(far)).start()
    for h in both:
        product = lax.dot_general(
            portion[h][...], portion[h][...], (((0,), (0,)), ((), ())), preferred_element_type=F32
        )
        new_right_stat[h] = decay_rate * right_stat[h] + (1.0 - decay_rate) / WIDTH * product
    places[0].take(FAR)
    every = scal_z.at[pl.ds(0, NZ * NY - 1)]
    send(every, every, szs, szr, at).wait_recv()
    total = scal_z[0]
    for k in range(1, NZ * NY):
        total = total + scal_z[k]
    scal_s[me] = total
    for step in range(1, NTP):
        send(scal_s.at[me], scal_s.at[me], sss, ssr, t_device(step)).start()
    places[1].take(FAR)
    send(stat_in, stat_in, lts, ltr, at).wait_recv()
    stat = stat_out[me]
    for far in range(NTP - 1):
        stat = stat + stat_in[far]
    new_left_stat[...] = decay_rate * left_stat[...] + (1.0 - decay_rate) / WIDTH * stat
    every = scal_s.at[pl.ds(0, NTP - 1)]
    send(every, every, sss, ssr, at).wait_recv()
    total = scal_s[0]
    for k in range(1, NTP):
        total = total + scal_s[k]
    factor = jnp.sqrt((total[:, HEAD // 2 : HEAD // 2 + 1] + epsilon) / (total[:, 0:1] + epsilon))
    for h in both:
        step_own = factor * precond[h]
        update_step[:, lanes[h]] = step_own
        new_weight[:, lanes[h]] = weight[:, lanes[h]] - learn_rate * step_own
    weights.wait_across()
    scale = learn_rate * factor
    for h in both:
        places[h].wait_across()
        for k in range(NZ):
            rows = pl.ds(k * HEAD, HEAD)
            held = held_weight[rows, lanes[h]].astype(F32)
            new_copy[rows, lanes[h]] = (held - scale * held_step[h][rows].astype(F32)).astype(BF)

    for h in both:
        every = partial_half[h].at[pl.ds(0, NZ * (NY - 1) * ROWS)]
        send(every, every, rys[h], ryr[h].at[0], at).wait_send()
        send(to_z[h], to_z[h], rzs[h], rzr[h], at).wait_send()
    every = scal_s.at[pl.ds(0, NTP - 1)]
    send(every, every, sss, ssr, at).wait_send()
    every = scal_z.at[pl.ds(0, NZ * NY - 1)]
    send(every, every, szs, szr, at).wait_send()
    send(stat_in, stat_in, lts, ltr, at).wait_send()
    for spread in (weights, *grads, *places):
        spread.drain()


def store(*refs):
    given, out, sem = refs[:5], refs[5:10], refs[10]
    copies = [pltpu.make_async_copy(a, b, sem.at[k]) for k, (a, b) in enumerate(zip(given, out))]
    for copy in copies:
        copy.start()
    for copy in copies:
        copy.wait()


def shards(
    cotangent,
    values_first,
    values_second,
    head_lambda,
    out_gain,
    weight,
    left_stat,
    right_stat,
    left_root,
    right_root,
):
    vmem = pl.BlockSpec(memory_space=pltpu.VMEM)
    anywhere = pl.BlockSpec(memory_space=pl.ANY)
    dma = pltpu.SemaphoreType.DMA
    spread = [dma, dma((len(GROUPS),)), dma, dma]
    given = (
        values_first,
        values_second,
        out_gain.reshape(1, HEAD),
        head_lambda,
        cotangent,
        weight,
        left_root,
        right_root,
        left_stat,
        right_stat,
    )
    local = [pltpu.SMEM(a.shape, F32) if a is head_lambda else pltpu.VMEM(a.shape, a.dtype) for a in given]

    def per_head(*shape):
        return [pltpu.VMEM((*shape, HEAD), BF)] * HEADS

    results = (
        jax.ShapeDtypeStruct((ROWS, COLS), F32),
        jax.ShapeDtypeStruct((ROWS, COLS), F32),
        jax.ShapeDtypeStruct((WIDTH, COLS), BF),
        jax.ShapeDtypeStruct((ROWS, COLS), F32),
        jax.ShapeDtypeStruct((COLS // HEAD, HEAD, HEAD), F32),
    )
    outs = pl.pallas_call(
        kernel,
        out_shape=results,
        in_specs=[pl.BlockSpec(memory_space=pltpu.HBM)] * 10,
        out_specs=[vmem] * 5,
        scratch_shapes=[
            *local,
            dma((10,)),
            pltpu.VMEM((128, COLS), BF),
            pltpu.VMEM((WIDTH, COLS), F32),
            *per_head(WIDTH),
            *per_head(NZ, NY - 1, ROWS),
            *per_head(NZ - 1, ROWS),
            *per_head(len(UP), ROWS),
            *per_head(len(DOWN), ROWS),
            *per_head(len(DIRECT), ROWS),
            pltpu.VMEM((WIDTH, COLS), BF),
            *per_head(WIDTH),
            *per_head(WIDTH),
            pltpu.VMEM((NTP, ROWS, COLS), F32),
            pltpu.VMEM((NTP - 1, ROWS, COLS), F32),
            pltpu.VMEM((NTP, 1, HEAD), F32),
            pltpu.VMEM((NZ * NY, 1, HEAD), F32),
            *[dma] * HEADS,
            *[dma((len(BATCH),))] * HEADS,
            *[dma] * (4 * HEADS),
            *spread,
            dma,
            *spread * (2 * HEADS),
            *[dma] * 6,
        ],
        compiler_params=pltpu.CompilerParams(
            collective_id=0, has_side_effects=True, vmem_limit_bytes=28 * 2**20
        ),
        name="fused",
    )(*[pltpu.with_memory_space_constraint(a, pltpu.HBM) for a in given])
    return pl.pallas_call(
        store,
        out_shape=results,
        in_specs=[vmem] * 5,
        out_specs=[anywhere] * 5,
        scratch_shapes=[dma((5,))],
        compiler_params=pltpu.CompilerParams(vmem_limit_bytes=8 * 2**20),
        name="store",
    )(*outs)


def solution(mesh):
    finer = Mesh(mesh.devices.reshape(NZ, NY, NX, NC), ("fs_0", "fs_1", "tp_0", "tp_1"))
    in_specs = (
        P(FS, None),
        P(FS, TP),
        P(FS, TP),
        P(TP),
        P(),
        P(FS, TP),
        P(FS, TP),
        P(TP, None, None),
        P(FS, None),
        P(TP, None, None),
    )
    out_specs = (P(FS, TP), P(FS, TP), P(None, TP), P(FS, TP), P(TP, None, None))
    return jax.shard_map(
        shards, mesh=finer, in_specs=in_specs, out_specs=out_specs, check_vma=False
    )
```

```python
import jax
import jax.numpy as jnp
from jax import lax
from jax.experimental import pallas as pl
from jax.experimental.pallas import tpu as pltpu
from jax.sharding import Mesh
from jax.sharding import PartitionSpec as P

TP = ("tp_0", "tp_1")
FS = ("fs_0", "fs_1")
NZ, NY, NX, NC = 16, 4, 4, 2
NTP = NX * NC
ROWS = 32
COLS = 256
HEAD = 128
WIDTH = 2048
REACH = 4
HEADS = COLS // HEAD
ORDER = (8, 7, 9, 6, 10, 5, 11, 4, 12, 3, 13, 2, 14, 1, 15, 0)
BATCH = ((8, 7), (9, 6), (10,), (5, 11), (4, 12), (3, 13), (2, 14), (1, 15), (0,))
UP, DOWN = (8, 7, 6, 5), (9, 10, 11)
DIRECT = (1, 15, 2, 14, 3, 13, 4, 12)
NEAR = ((1, 15), (2, 14), (3, 13))
MID = ((4,), (12,))
FAR = ((5, 11), (6, 10), (7, 9), (8,))
GROUPS = NEAR + MID + FAR
GROUP_OF = {step: k for k, group in enumerate(GROUPS) for step in group}

epsilon = 1e-06
decay_rate = 0.9
learn_rate = 0.01
output_scale = 0.2

BF = jnp.bfloat16
F32 = jnp.float32


def rows_of(z, y):
    return pl.ds(pl.multiple_of(z * (NY * ROWS) + y * ROWS, ROWS), ROWS)


def around(position, step, size):
    return lax.rem(position + (step % size), size)


def send(src, dst, send_sem, recv_sem, device):
    return pltpu.make_async_remote_copy(
        src_ref=src,
        dst_ref=dst,
        send_sem=send_sem,
        recv_sem=recv_sem,
        device_id=device,
        device_id_type=pl.DeviceIdType.MESH,
    )


class Spread:
    def __init__(self, buf, sems, at, slow=False):
        self.buf = buf
        self.zs, self.zr, self.ys, self.yr, self.ya = sems
        self.at = at
        self.slow = slow

    def block(self, step):
        z, y, x, c = self.at
        return self.buf.at[rows_of(around(z, -step, NZ), y)]

    def whole(self, blocks):
        return self.buf.at[pl.ds(0, blocks * ROWS)]

    def launch(self, step, reach, down):
        z, y, x, c = self.at
        block = self.block(step)
        there = around(z, -reach if down else reach, NZ)
        arrives = (step - reach if down else step + reach) % NZ
        send(block, block, self.zs, self.zr.at[GROUP_OF[arrives]], (there, y, x, c)).start()

    def begin(self):
        for reach in (1, 4, 2, 3):
            self.launch(0, reach, False)
            self.launch(0, reach, True)

    def wait(self, group):
        every = self.whole(len(group))
        send(every, every, self.zs, self.zr.at[GROUP_OF[group[0]]], self.at).wait_recv()

    def relay(self):
        for reach in (1, 2, 3, 4):
            self.launch(4, reach, False)
            if reach < 4:
                self.launch(12, reach, True)

    def to_y(self, block, far, sem):
        z, y, x, c = self.at
        send(block, block, self.ys, sem, (z, around(y, far, NY), x, c)).start()

    def across(self, group):
        for step in group:
            block = self.block(step)
            if self.slow:
                onward = 3 if step % 2 else 1
                self.to_y(block, onward, self.ya)
                self.to_y(block, NY - onward, self.yr)
            else:
                for far in (2, 1, 3):
                    self.to_y(block, far, self.yr)

    def take(self, groups):
        for group in groups:
            self.wait(group)
            self.across(group)

    def onward(self):
        z, y, x, c = self.at
        every = self.whole(NZ)
        send(every, every, self.ys, self.ya, self.at).wait_recv()
        for step in range(NZ):
            far = 3 if step % 2 else 1
            block = self.buf.at[rows_of(around(z, -step, NZ), around(y, -far, NY))]
            self.to_y(block, far, self.yr)

    def wait_across(self):
        every = self.whole(NZ * (2 if self.slow else 3))
        send(every, every, self.ys, self.yr, self.at).wait_recv()

    def drain(self):
        every = self.whole(NZ * (NY - 1))
        send(every, every, self.ys, self.yr, self.at).wait_send()
        every = self.whole(NZ - 1)
        send(every, every, self.zs, self.zr.at[0], self.at).wait_send()


def kernel(*refs):
    refs = list(refs)

    def grab(count):
        taken = refs[:count]
        del refs[:count]
        return taken

    sources = grab(10)
    update_step, new_weight, new_copy, new_left_stat, new_right_stat = grab(5)
    local = grab(10)
    first, second, gain, lam, cot, weight, left_root, right_root, left_stat, right_stat = local
    (load_sem,) = grab(1)
    head_out, partial = grab(2)
    partial_half, from_y, to_z, from_up, from_down, from_z = (grab(HEADS) for _ in range(6))
    (held_weight,) = grab(1)
    portion, held_step = grab(HEADS), grab(HEADS)
    stat_out, stat_in, scal_s, scal_z = grab(4)
    rys, ryr, rzs, rzr, rup, rdown = (grab(HEADS) for _ in range(6))
    wsems = grab(5)
    gsems = [[*grab(4), None] for _ in range(HEADS)]
    psems = [[*grab(4), None] for _ in range(HEADS)]
    sss, ssr, szs, szr, lts, ltr = grab(6)

    z, y, x, c = (lax.axis_index(a) for a in ("fs_0", "fs_1", "tp_0", "tp_1"))
    at = (z, y, x, c)
    me = x * NC + c
    both = range(HEADS)
    lanes = [slice(h * HEAD, (h + 1) * HEAD) for h in both]

    def z_device(step):
        return (around(z, step, NZ), y, x, c)

    def y_device(step):
        return (z, around(y, step, NY), x, c)

    def t_index(step):
        return around(me, step, NTP)

    def t_device(step):
        other = t_index(step)
        return (z, y, other // NC, lax.rem(other, NC))

    barrier = pltpu.get_barrier_semaphore()
    peers = [z_device(s) for s in DIRECT] + [y_device(s) for s in range(1, NY)]
    peers += [t_device(s) for s in range(1, NTP)]
    for peer in peers:
        pl.semaphore_signal(barrier, inc=1, device_id=peer, device_id_type=pl.DeviceIdType.MESH)

    loads = [pltpu.make_async_copy(a, b, load_sem.at[k]) for k, (a, b) in enumerate(zip(sources, local))]
    for load in loads:
        load.start()
    for load in loads[:4]:
        load.wait()
    for h in both:
        difference = first[:, lanes[h]].astype(F32) - lam[h] * second[:, lanes[h]].astype(F32)
        mean = jnp.mean(difference * difference, axis=-1, keepdims=True)
        scaled = difference * lax.rsqrt(mean + epsilon) * gain[...] * output_scale
        head_out[:, lanes[h]] = scaled.astype(BF)

    def chunk(step):
        zz = around(z, step, NZ)
        rows = pl.ds(pl.multiple_of(zz * HEAD, HEAD), HEAD)
        block = lax.dot_general(
            cot[:, rows], head_out[...], (((0,), (0,)), ((), ())), preferred_element_type=F32
        )
        partial[rows] = block
        for h in both:
            partial_half[h][rows] = block[:, lanes[h]].astype(BF)

    batch_of = {step: k for k, group in enumerate(BATCH) for step in group}
    spot = {step: k for k, step in enumerate(step for group in BATCH for step in group)}

    def chunk_out(h, step):
        zz = around(z, step, NZ)
        for far in (2, 1, 3):
            send(
                partial_half[h].at[rows_of(zz, around(y, far, NY))],
                from_y[h].at[spot[step], far - 1],
                rys[h],
                ryr[h].at[batch_of[step]],
                y_device(far),
            ).start()

    loads[4].wait()
    for step in ORDER:
        chunk(step)
    loads[5].wait()
    held_weight[rows_of(z, y)] = weight[...].astype(BF)

    pl.semaphore_wait(barrier, len(peers))

    for h in both:
        for step in ORDER[:7]:
            chunk_out(h, step)
    weights = Spread(held_weight, wsems, at, True)
    weights.begin()
    for step in ORDER[7:]:
        chunk_out(0, step)
    for step in ORDER[7:]:
        chunk_out(1, step)

    def arrive(h, group):
        block = from_y[h].at[pl.ds(spot[group[0]], len(group))]
        send(block, block, rys[h], ryr[h].at[batch_of[group[0]]], at).wait_recv()

    def summed(h, step):
        total = partial[rows_of(around(z, step, NZ), y), lanes[h]]
        for far in range(NY - 1):
            total = total + from_y[h][spot[step], far].astype(F32)
        return total

    slot = {step: k for k, step in enumerate(DIRECT)}

    def pass_on(h, groups):
        for group in groups:
            arrive(h, group)
            for step in group:
                out = to_z[h].at[step - 1]
                to_z[h][step - 1] = summed(h, step).astype(BF)
                if step in UP:
                    send(out, from_up[h].at[UP.index(step)], rzs[h], rup[h], z_device(step - REACH)).start()
                elif step in DOWN:
                    send(out, from_down[h].at[DOWN.index(step)], rzs[h], rdown[h], z_device(step + REACH)).start()
                else:
                    send(out, from_z[h].at[slot[step]], rzs[h], rzr[h], z_device(step)).start()

    def combine(h):
        arrive(h, BATCH[4])
        for far, given, sem in ((4, from_up[h], rup[h]), (12, from_down[h], rdown[h])):
            total = summed(h, far)
            send(given, given, rzs[h], sem, at).wait_recv()
            for k in range(given.shape[0]):
                total = total + given[k].astype(F32)
            to_z[h][far - 1] = total.astype(BF)
            send(to_z[h].at[far - 1], from_z[h].at[slot[far]], rzs[h], rzr[h], z_device(far)).start()

    def finish(h):
        arrive(h, BATCH[8])
        own = summed(h, 0)
        send(from_z[h], from_z[h], rzs[h], rzr[h], at).wait_recv()
        for k in range(len(DIRECT)):
            own = own + from_z[h][k].astype(F32)
        return own

    pass_on(0, BATCH[:4])
    pass_on(1, BATCH[:4])
    combine(0)
    pass_on(0, BATCH[5:8])
    combine(1)
    pass_on(1, BATCH[5:8])
    own, own_half, grads = [None] * HEADS, [None] * HEADS, [None] * HEADS

    def gather(h):
        own[h] = finish(h)
        own_half[h] = own[h].astype(BF)
        portion[h][rows_of(z, y)] = own_half[h]
        grads[h] = Spread(portion[h], gsems[h], at)
        grads[h].begin()
        grads[h].across((0,))

    gather(0)
    weights.across((0,))
    for group in NEAR + MID:
        weights.wait(group)
    for group in NEAR + MID:
        weights.across(group)
    for load in loads[6:]:
        load.wait()
    gather(1)
    grads[0].take(NEAR)
    for group in MID:
        grads[0].wait(group)
    grads[0].relay()
    for group in MID:
        grads[0].across(group)
    grads[1].take(NEAR)
    for group in MID:
        grads[1].wait(group)
    grads[1].relay()
    weights.relay()
    for group in MID:
        grads[1].across(group)
    grads[0].take(FAR)
    grads[1].take(FAR)

    precond, places = [None] * HEADS, [None] * HEADS

    def send_squares():
        squares = [jnp.sum(v * v, axis=(0, 1), keepdims=True) for v in (*precond, *own)]
        low = lax.broadcasted_iota(jnp.int32, (1, HEAD), 1) < HEAD // 2
        mine = z * NY + y
        scal_z[mine] = jnp.where(low, squares[0] + squares[1], squares[2] + squares[3])
        for step in ORDER:
            for up in (2, 1, 3, 0):
                if step or up:
                    there = (around(z, step, NZ), around(y, up, NY), x, c)
                    send(scal_z.at[mine], scal_z.at[mine], szs, szr, there).start()

    def advance(h):
        left_half = jnp.dot(left_root[...], portion[h][...], preferred_element_type=F32).astype(BF)
        precond[h] = jnp.dot(left_half, right_root[h], preferred_element_type=F32)
        if h == HEADS - 1:
            send_squares()
        held_step[h][rows_of(z, y)] = precond[h].astype(BF)
        places[h] = Spread(held_step[h], psems[h], at)
        places[h].begin()
        places[h].across((0,))

    grads[0].wait_across()
    advance(0)
    weights.take(FAR)
    grads[1].wait_across()
    advance(1)
    places[0].take(NEAR)
    for group in MID:
        places[0].wait(group)
    places[0].relay()
    for group in MID:
        places[0].across(group)

    weights.onward()
    places[1].take(NEAR)
    for group in MID:
        places[1].wait(group)
    places[1].relay()
    for group in MID:
        places[1].across(group)
    contract = (((1,), (1,)), ((), ()))
    for j in range(NTP):
        rows = slice(j * COLS, (j + 1) * COLS)
        stat_out[j] = sum(
            lax.dot_general(own_half[h], portion[h][rows], contract, preferred_element_type=F32)
            for h in both
        )
    for far in range(1, NTP):
        send(stat_out.at[t_index(far)], stat_in.at[far - 1], lts, ltr, t_device(far)).start()
    for h in both:
        product = lax.dot_general(
            portion[h][...], portion[h][...], (((0,), (0,)), ((), ())), preferred_element_type=F32
        )
        new_right_stat[h] = decay_rate * right_stat[h] + (1.0 - decay_rate) / WIDTH * product
    places[0].take(FAR)
    every = scal_z.at[pl.ds(0, NZ * NY - 1)]
    send(every, every, szs, szr, at).wait_recv()
    total = scal_z[0]
    for k in range(1, NZ * NY):
        total = total + scal_z[k]
    scal_s[me] = total
    for step in range(1, NTP):
        send(scal_s.at[me], scal_s.at[me], sss, ssr, t_device(step)).start()
    places[1].take(FAR)
    send(stat_in, stat_in, lts, ltr, at).wait_recv()
    stat = stat_out[me]
    for far in range(NTP - 1):
        stat = stat + stat_in[far]
    new_left_stat[...] = decay_rate * left_stat[...] + (1.0 - decay_rate) / WIDTH * stat
    every = scal_s.at[pl.ds(0, NTP - 1)]
    send(every, every, sss, ssr, at).wait_recv()
    total = scal_s[0]
    for k in range(1, NTP):
        total = total + scal_s[k]
    factor = jnp.sqrt((total[:, HEAD // 2 : HEAD // 2 + 1] + epsilon) / (total[:, 0:1] + epsilon))
    for h in both:
        step_own = factor * precond[h]
        update_step[:, lanes[h]] = step_own
        new_weight[:, lanes[h]] = weight[:, lanes[h]] - learn_rate * step_own
    weights.wait_across()
    scale = learn_rate * factor
    for h in both:
        places[h].wait_across()
        for k in range(NZ):
            rows = pl.ds(k * HEAD, HEAD)
            held = held_weight[rows, lanes[h]].astype(F32)
            new_copy[rows, lanes[h]] = (held - scale * held_step[h][rows].astype(F32)).astype(BF)

    for h in both:
        every = partial_half[h].at[pl.ds(0, NZ * (NY - 1) * ROWS)]
        send(every, every, rys[h], ryr[h].at[0], at).wait_send()
        send(to_z[h], to_z[h], rzs[h], rzr[h], at).wait_send()
    every = scal_s.at[pl.ds(0, NTP - 1)]
    send(every, every, sss, ssr, at).wait_send()
    every = scal_z.at[pl.ds(0, NZ * NY - 1)]
    send(every, every, szs, szr, at).wait_send()
    send(stat_in, stat_in, lts, ltr, at).wait_send()
    for spread in (weights, *grads, *places):
        spread.drain()


def store(*refs):
    given, out, sem = refs[:5], refs[5:10], refs[10]
    copies = [pltpu.make_async_copy(a, b, sem.at[k]) for k, (a, b) in enumerate(zip(given, out))]
    for copy in copies:
        copy.start()
    for copy in copies:
        copy.wait()


def shards(
    cotangent,
    values_first,
    values_second,
    head_lambda,
    out_gain,
    weight,
    left_stat,
    right_stat,
    left_root,
    right_root,
):
    vmem = pl.BlockSpec(memory_space=pltpu.VMEM)
    anywhere = pl.BlockSpec(memory_space=pl.ANY)
    dma = pltpu.SemaphoreType.DMA
    spread = [dma, dma((len(GROUPS),)), dma, dma]
    given = (
        values_first,
        values_second,
        out_gain.reshape(1, HEAD),
        head_lambda,
        cotangent,
        weight,
        left_root,
        right_root,
        left_stat,
        right_stat,
    )
    local = [pltpu.SMEM(a.shape, F32) if a is head_lambda else pltpu.VMEM(a.shape, a.dtype) for a in given]

    def per_head(*shape):
        return [pltpu.VMEM((*shape, HEAD), BF)] * HEADS

    results = (
        jax.ShapeDtypeStruct((ROWS, COLS), F32),
        jax.ShapeDtypeStruct((ROWS, COLS), F32),
        jax.ShapeDtypeStruct((WIDTH, COLS), BF),
        jax.ShapeDtypeStruct((ROWS, COLS), F32),
        jax.ShapeDtypeStruct((COLS // HEAD, HEAD, HEAD), F32),
    )
    outs = pl.pallas_call(
        kernel,
        out_shape=results,
        in_specs=[pl.BlockSpec(memory_space=pltpu.HBM)] * 10,
        out_specs=[vmem] * 5,
        scratch_shapes=[
            *local,
            dma((10,)),
            pltpu.VMEM((128, COLS), BF),
            pltpu.VMEM((WIDTH, COLS), F32),
            *per_head(WIDTH),
            *per_head(NZ, NY - 1, ROWS),
            *per_head(NZ - 1, ROWS),
            *per_head(len(UP), ROWS),
            *per_head(len(DOWN), ROWS),
            *per_head(len(DIRECT), ROWS),
            pltpu.VMEM((WIDTH, COLS), BF),
            *per_head(WIDTH),
            *per_head(WIDTH),
            pltpu.VMEM((NTP, ROWS, COLS), F32),
            pltpu.VMEM((NTP - 1, ROWS, COLS), F32),
            pltpu.VMEM((NTP, 1, HEAD), F32),
            pltpu.VMEM((NZ * NY, 1, HEAD), F32),
            *[dma] * HEADS,
            *[dma((len(BATCH),))] * HEADS,
            *[dma] * (4 * HEADS),
            *spread,
            dma,
            *spread * (2 * HEADS),
            *[dma] * 6,
        ],
        compiler_params=pltpu.CompilerParams(
            collective_id=0, has_side_effects=True, vmem_limit_bytes=28 * 2**20
        ),
        name="fused",
    )(*[pltpu.with_memory_space_constraint(a, pltpu.HBM) for a in given])
    return pl.pallas_call(
        store,
        out_shape=results,
        in_specs=[vmem] * 5,
        out_specs=[anywhere] * 5,
        scratch_shapes=[dma((5,))],
        compiler_params=pltpu.CompilerParams(vmem_limit_bytes=8 * 2**20),
        name="store",
    )(*outs)


def solution(mesh):
    finer = Mesh(mesh.devices.reshape(NZ, NY, NX, NC), ("fs_0", "fs_1", "tp_0", "tp_1"))
    in_specs = (
        P(FS, None),
        P(FS, TP),
        P(FS, TP),
        P(TP),
        P(),
        P(FS, TP),
        P(FS, TP),
        P(TP, None, None),
        P(FS, None),
        P(TP, None, None),
    )
    out_specs = (P(FS, TP), P(FS, TP), P(None, TP), P(FS, TP), P(TP, None, None))
    return jax.shard_map(
        shards, mesh=finer, in_specs=in_specs, out_specs=out_specs, check_vma=False
    )
```
